256 devices in a mesh: ep: 64 (over z, y, core), tp: 4 (over x).
Axes of the slice: x: 4, y: 4, z: 8, core: 2. Of those that a mesh axis runs over, the one named last changes fastest.
Arguments:
- first_input: bfloat16 [32768, 2048], P('ep'), may hold values from -120 to 120
- first_gain: bfloat16 [2048], replicated, may hold values from 0.099609375 to 1.8984375
- pool_inward: bfloat16 [2048, 1024], P(None, 'tp'), may hold values from -0.125 to 0.125
- pool_mixing: bfloat16 [4, 256, 256], P('tp'), may hold values from -0.375 to 0.375
- pool_scale: bfloat16 [1024], P('tp'), may hold values from 0.099609375 to 1.8984375
- pool_outward: bfloat16 [1024, 2048], P('tp'), may hold values from -0.1875 to 0.1875
- second_input: bfloat16 [16384, 2048], P('ep'), may hold values from -120 to 120
- second_gain: bfloat16 [2048], replicated, may hold values from 0.099609375 to 1.8984375
- route_ids: int32 [16384, 2], P('ep'), may hold values from 0 to 31, all different within a row; in each aligned block of 256 rows (0 to 255, 256 to 511, ...) at most 18 rows name the same one
- route_logits: float32 [16384, 2], P('ep'), may hold values from -6 to 6
- expert_gate: bfloat16 [64, 2048, 2048], P('ep', None, 'tp'), may hold values from -0.125 to 0.125
- expert_up: bfloat16 [64, 2048, 2048], P('ep', None, 'tp'), may hold values from -0.125 to 0.125
- expert_down: bfloat16 [64, 2048, 2048], P('ep', 'tp'), may hold values from -0.09375 to 0.09375
Outputs:
- first_out: bfloat16 [32768, 2048], P('ep', 'tp')
- second_out: bfloat16 [16384, 2048], P('ep', 'tp')
The draws below stay inside these ranges and needn't reach their ends.
Inputs may be any that keep to these rules, and one draw needn't show every extreme that they name: `route_ids`: each row names two different experts. In each aligned block of 256 rows (the rows of one index of ep) no expert is named by more than 18 rows, and in some blocks one expert is named by exactly 18 rows.
All inputs are finite; a program needn't handle non-finite values.
Results may differ from the reference program's by a relative error of at most 0.012.
Values may be sent and summed in bfloat16 or wider, within the bound.
A program may use at most 64 MiB of HBM per device.

```python
import math
import jax
import jax.numpy as jnp
import numpy as np
from jax import lax

D = 2048
POOL = 1024
FF_E = 4096
B_ROWS = 256
EXPERTS = 32
CAP = 18
TOK_A = 32768
TOK_B = 16384
N_EP = 64
N_TP = 4


def scaled_rows(key, row_count, width):
    subkeys = jax.random.split(key, 3)
    column_scale = jnp.exp(jax.random.uniform(subkeys[1], (1, width), jnp.float32, 0.0, math.log(10.0)))
    row_scale = jnp.exp(jax.random.uniform(subkeys[2], (row_count, 1), jnp.float32, 0.0, math.log(10.0)))
    values = jax.random.truncated_normal(subkeys[0], -4.0, 4.0, (row_count, width), jnp.float32)
    return (values * column_scale * row_scale * 0.25).astype(jnp.bfloat16)


def draw_first_input(key, part):
    return scaled_rows(jax.random.fold_in(key, 11), TOK_A, D)


def draw_second_input(key, part):
    return scaled_rows(jax.random.fold_in(key, 23), TOK_B, D)


def levels(own_key, extent, cuts, least, high):
    def one(position, blocks):
        steps = jax.random.uniform(jax.random.fold_in(jax.random.fold_in(own_key, 6), position), (blocks,), jnp.float32, least / len(cuts), high / len(cuts))
        return jnp.repeat(jnp.exp(steps), extent[position] // blocks).reshape((-1,) + (1,) * (len(extent) - position - 1))

    loudness = one(*cuts[0])
    for cut in cuts[1:]:
        loudness = loudness * one(*cut)
    return loudness


def assign_block(rng, own, number, rows, amount, top, reach, skew):
    order = jax.random.permutation(rng, amount)
    packed, ordinary = portions_of(amount, rows * top, reach, skew, True), portions_of(amount, rows * top, reach, skew, False)
    places = jnp.arange(amount)

    def named(tallies, turn):
        used = int((tallies > 0).sum())
        fixed = max(1, used // 4)
        shifted = fixed + (places - fixed + turn * (used - fixed)) % max(1, amount - fixed)
        return jnp.zeros((amount,), jnp.int32).at[order[jnp.where(places < fixed, places, shifted)]].set(jnp.asarray(tallies, jnp.int32))

    tallies = jnp.where(number % 4 == 0, named(packed, number // 4), named(ordinary, number - number // 4 - 1))
    mixed = jax.random.permutation(jax.random.fold_in(own, 3), amount)
    donor, sink = mixed[0:amount // 2 * 2:2], mixed[1:amount // 2 * 2:2]
    slack = jnp.minimum(tallies[donor] - 1, reach - tallies[sink]) // 2
    slack = jnp.where((donor == order[0]) | (sink == order[0]) | (tallies[sink] == 0), 0, jnp.maximum(slack, 0))
    shifted = jax.random.randint(jax.random.fold_in(own, 4), (amount // 2,), 0, 1 << 20) % (slack + 1)
    tallies = tallies.at[donor].add(-shifted).at[sink].add(shifted)
    items = jnp.searchsorted(jnp.cumsum(tallies), jnp.arange(rows * top), side="right").astype(jnp.int32)
    listing = items.reshape(top, rows).T
    listing = listing[jax.random.permutation(jax.random.fold_in(own, 1), rows)]
    turn = jax.random.randint(jax.random.fold_in(own, 2), (rows, 1), 0, top)
    return jnp.take_along_axis(listing, (jnp.arange(top)[None, :] + turn) % top, axis=1)


def portions_of(count, total, most, slope, full):
    portions = [(1 << 20) // math.isqrt(grade ** slope) + 1 for grade in range(1, count + 1)]
    largest = most if full else min(most, max(-(-total // count), total * portions[0] // sum(portions)))
    least = 1 if total - largest >= count - 1 else 0
    given, surplus = [largest] + [least] * (count - 1), total - largest - least * (count - 1)
    while surplus > 0:
        free = [i for i in range(1, count) if given[i] < largest] or [i for i in range(1, count) if given[i] < most]
        whole, left = sum([portions[i] for i in free]), surplus
        for i in free:
            extra = min(most - given[i], max(1, left * portions[i] // whole), surplus)
            given[i] = given[i] + extra
            surplus = surplus - extra
    return np.array(given)


def noise(rng, extent, scale, most, pieces=(), kind=jnp.bfloat16):
    array = scale * jax.random.normal(rng, extent, jnp.float32)
    if pieces:
        array = array * levels(rng, extent, pieces, -0.22, 0.18)
    return jnp.clip(array, -most, most).astype(kind)


def setup_inputs(seed: int = 0) -> dict:
    seeds = jax.random.split(jax.random.key(seed), 14)
    first_input = draw_first_input(jax.random.fold_in(seeds[13], 71), 0)
    first_gain = jnp.clip(1.0 + 0.18 * jax.random.normal(seeds[1], (D,), jnp.float32), 0.099609375, 1.8984375).astype(jnp.bfloat16)
    pool_inward = noise(seeds[2], (D, POOL), D ** -0.5, 0.125, ((1, 4),))
    pool_mixing = noise(seeds[3], (4, POOL // 4, POOL // 4), (POOL // 4) ** -0.5, 0.375, ((0, 4),))
    pool_scale = jnp.clip(1.0 + 0.18 * jax.random.normal(seeds[4], (POOL,), jnp.float32), 0.099609375, 1.8984375).astype(jnp.bfloat16)
    pool_outward = noise(seeds[5], (POOL, D), POOL ** -0.5, 0.1875, ((0, 4),))
    second_input = draw_second_input(jax.random.fold_in(seeds[13], 71), 0)
    second_gain = jnp.clip(1.0 + 0.18 * jax.random.normal(seeds[7], (D,), jnp.float32), 0.099609375, 1.8984375).astype(jnp.bfloat16)
    route_ids_keys = jax.random.split(jax.random.fold_in(seeds[8], 1), TOK_B // B_ROWS)
    route_ids_turns = jax.random.permutation(jax.random.fold_in(seeds[8], 3), TOK_B // B_ROWS)
    route_ids = jax.vmap(lambda own, number: assign_block(jax.random.fold_in(seeds[8], 2), own, number, B_ROWS, EXPERTS, 2, CAP, 0))(route_ids_keys, route_ids_turns).reshape((TOK_B, 2))
    route_logits = noise(seeds[9], (TOK_B, 2), 1.5, 6.0, ((0, 64),), jnp.float32)
    expert_gate = noise(seeds[10], (2 * EXPERTS, D, FF_E // 2), D ** -0.5, 0.125, ((0, 64), (2, 4)))
    expert_up = noise(seeds[11], (2 * EXPERTS, D, FF_E // 2), D ** -0.5, 0.125, ((0, 64), (2, 4)))
    expert_down = noise(seeds[12], (2 * EXPERTS, FF_E // 2, D), FF_E ** -0.5, 0.09375, ((0, 64), (1, 4)))
    return dict(first_input=first_input, first_gain=first_gain, pool_inward=pool_inward, pool_mixing=pool_mixing, pool_scale=pool_scale, pool_outward=pool_outward, second_input=second_input, second_gain=second_gain, route_ids=route_ids, route_logits=route_logits, expert_gate=expert_gate, expert_up=expert_up, expert_down=expert_down)


epsilon = 1e-06
window_lengths = (2, 4, 8, 16)

def rms_scaled(values, weights):
    widened = values.astype(jnp.float32)
    inverse = lax.rsqrt(lax.optimization_barrier(jnp.mean(widened * widened, axis=-1, keepdims=True)) + epsilon)
    return (widened * inverse * weights.astype(jnp.float32)).astype(jnp.bfloat16)

def window_means(channels, length, offset):
    row_count = channels.shape[0] - 15
    summed = jnp.zeros((row_count, channels.shape[1]), jnp.float32)
    for lookback in range(16):
        summed = summed + jnp.where(lookback < length, channels[15 - lookback:15 - lookback + row_count], 0.0)
    positions = offset + jnp.arange(row_count, dtype=jnp.int32)
    counts = jnp.minimum(positions + 1, length).astype(jnp.float32)
    return summed / counts[:, None]

def slot_positions(block_ids, expert_count, capacity):
    flattened = block_ids.reshape(-1)
    onehot = (flattened[:, None] == jnp.arange(expert_count, dtype=jnp.int32)[None, :]).astype(jnp.int32)
    running = jnp.cumsum(onehot, axis=0, dtype=jnp.int32) - 1
    slot_numbers = lax.optimization_barrier(jnp.sum(onehot * running, axis=1))
    return (flattened * capacity + slot_numbers).astype(jnp.int32)

def mixer_half(first_input, first_gain, pool_inward, pool_mixing, pool_scale, pool_outward):
    normed = rms_scaled(first_input, first_gain)
    pooled_in = jnp.dot(normed, pool_inward, preferred_element_type=jnp.float32).astype(jnp.bfloat16)
    group_width = pool_inward.shape[1] // 4
    accumulated = jnp.zeros(first_input.shape, jnp.float32)
    for group_index in range(4):
        lower = group_index * group_width
        channels = pooled_in[:, lower:lower + group_width]
        widened = jnp.pad(channels.astype(jnp.float32), ((15, 0), (0, 0)))
        means = window_means(widened, window_lengths[group_index], jnp.int32(0))
        mixed = (means - channels.astype(jnp.float32)).astype(jnp.bfloat16)
        scales = pool_scale[lower:lower + group_width].astype(jnp.float32)
        pooled = (jnp.dot(mixed, pool_mixing[group_index], preferred_element_type=jnp.float32) * scales).astype(jnp.bfloat16)
        partial_value = jnp.dot(pooled, pool_outward[lower:lower + group_width], preferred_element_type=jnp.float32).astype(jnp.bfloat16)
        accumulated = accumulated + partial_value.astype(jnp.float32)
    return accumulated.astype(jnp.bfloat16)

def block_tables(block_positions, block_shares, first_token):
    tokens = first_token + jnp.arange(2 * B_ROWS, dtype=jnp.int32) // 2
    owners = jnp.zeros((EXPERTS * CAP,), jnp.int32).at[block_positions].set(tokens)
    weights = jnp.zeros((EXPERTS * CAP,), jnp.float32).at[block_positions].set(block_shares)
    return (owners, weights)

def block_slots(block_ids):
    return slot_positions(block_ids, EXPERTS, CAP)

def expert_half(second_input, second_gain, route_ids, route_logits, expert_gate, expert_up, expert_down):
    normed = rms_scaled(second_input, second_gain)
    positions = jax.vmap(block_slots)(route_ids.reshape(N_EP, B_ROWS, 2))
    shares = jax.nn.sigmoid(route_logits - route_logits[:, ::-1])
    starts = jnp.arange(N_EP, dtype=jnp.int32) * B_ROWS
    owners, weights = jax.vmap(block_tables)(positions, shares.reshape(N_EP, 2 * B_ROWS), starts)
    owners = owners.reshape(N_EP, EXPERTS, CAP).transpose(1, 0, 2).reshape(EXPERTS, N_EP * CAP)
    weights = weights.reshape(N_EP, EXPERTS, CAP).transpose(1, 0, 2).reshape(EXPERTS, N_EP * CAP)
    half_units = expert_gate.shape[2]
    unit_group = half_units // N_TP
    gate_pairs = expert_gate.reshape(EXPERTS, 2, D, half_units)
    up_pairs = expert_up.reshape(EXPERTS, 2, D, half_units)
    down_pairs = expert_down.reshape(EXPERTS, 2, half_units, D)

    def add_expert(accumulated, inputs):
        slot_owners, slot_weights, gate_pair, up_pair, down_pair = inputs
        routed = normed[slot_owners]
        gate_full = jnp.concatenate([gate_pair[0], gate_pair[1]], axis=1)
        up_full = jnp.concatenate([up_pair[0], up_pair[1]], axis=1)
        gate_sum = jnp.dot(routed, gate_full, preferred_element_type=jnp.float32)
        up_sum = jnp.dot(routed, up_full, preferred_element_type=jnp.float32)
        hidden = (jax.nn.silu(gate_sum) * up_sum).astype(jnp.bfloat16)
        down_full = down_pair.reshape(2 * half_units, D)
        route_out = jnp.zeros((routed.shape[0], D), jnp.float32)
        for half_index in range(2):
            half_sum = jnp.zeros((routed.shape[0], D), jnp.float32)
            for quarter in range(N_TP):
                first_unit = half_index * half_units + quarter * unit_group
                product = jnp.dot(hidden[:, first_unit:first_unit + unit_group], down_full[first_unit:first_unit + unit_group], preferred_element_type=jnp.float32).astype(jnp.bfloat16)
                half_sum = half_sum + product.astype(jnp.float32)
            route_out = route_out + half_sum.astype(jnp.bfloat16).astype(jnp.float32)
        return (accumulated.at[slot_owners].add(slot_weights[:, None] * route_out), None)
    accumulated, unused = lax.scan(add_expert, jnp.zeros((second_input.shape[0], D), jnp.float32), (owners, weights, gate_pairs, up_pairs, down_pairs))
    return accumulated.astype(jnp.bfloat16)

def reference(first_input, first_gain, pool_inward, pool_mixing, pool_scale, pool_outward, second_input, second_gain, route_ids, route_logits, expert_gate, expert_up, expert_down):
    first_out = mixer_half(first_input, first_gain, pool_inward, pool_mixing, pool_scale, pool_outward)
    second_out = expert_half(second_input, second_gain, route_ids, route_logits, expert_gate, expert_up, expert_down)
    return (first_out, second_out)
```

```python
import jax
import jax.numpy as jnp
from jax import lax
from jax.experimental import pallas as pl
from jax.experimental.pallas import tpu as pltpu
from jax.sharding import PartitionSpec as P

MESH = pl.DeviceIdType.MESH
F32, BF16 = jnp.float32, jnp.bfloat16
EPS = 1e-06
ZN, YN, XN = 8, 4, 4
NB = ZN * YN
NG = ZN
EP = NB * 2
HALF = NB // 2


def dot(a, b):
    return jnp.dot(a, b, preferred_element_type=F32)


def dot_t(a, b):
    return lax.dot_general(a, b, (((0,), (0,)), ((), ())), preferred_element_type=F32)


def iota(shape, dim):
    return lax.broadcasted_iota(jnp.int32, shape, dim)


def group_dz(g):
    return jnp.where((g & 1) == 1, (g + 1) >> 1, (8 - (g >> 1)) & 7)


def kernel(
    x1_h, g1, pin_h, pmix, psc, pout_h, x2_h, g2, ids, lg, wg_h, wu_h, wd_h,
    out1, out2,
    x1, pin, x2, wg, wu, wd, wg2, wu2, wd2,
    n1, pl_in, ext, halo, tail, plx, wo, xq,
    s, r, lhs, hid, tm, rr, fin, ret, fm, fo,
    sem_in, ws_s, ws_r, a_s, a_r, g_s, g_r, t_s, t_r, b_s, b_r, h_s, h_r, wo_s, wo_r, wp_s, wp_r, p_s, p_r,
):
    ep, t = lax.axis_index("ep"), lax.axis_index("tp")
    c = lax.rem(ep, 2)
    chip = ep // 2
    y, z = lax.rem(chip, YN), chip // YN

    def at(dz, dy, dc=0):
        z2, y2, c2 = lax.rem(z + dz + ZN, ZN), lax.rem(y + dy + YN, YN), lax.rem(c + dc, 2)
        return ((z2 * YN + y2) * 2 + c2, t)

    def along(dx):
        return (ep, lax.rem(t + dx, XN))

    partner = at(0, 0, 1)
    following = (lax.rem(ep + 1, EP), t)
    previous = (lax.rem(ep + EP - 1, EP), t)

    def remote(src, dst, ss, rs, device):
        return pltpu.make_async_remote_copy(
            src_ref=src, dst_ref=dst, send_sem=ss, recv_sem=rs, device_id=device, device_id_type=MESH
        )

    loads = [
        pltpu.make_async_copy(a, b, sem_in.at[i])
        for i, (a, b) in enumerate(
            [(x2_h, x2), (x1_h, x1), (pin_h, pin), (wg_h.at[0], wg), (wu_h.at[0], wu), (wd_h.at[0], wd)]
        )
    ]
    for copy in loads:
        copy.start()

    bar = pltpu.get_barrier_semaphore()

    def greet(b, carry):
        pl.semaphore_signal(bar, inc=1, device_id=at(b // YN, lax.rem(b, YN)), device_id_type=MESH)
        return carry

    lax.fori_loop(1, NB, greet, 0)
    for dx in (1, 2, 3):
        pl.semaphore_signal(bar, inc=1, device_id=along(dx), device_id_type=MESH)
    pl.semaphore_signal(bar, inc=1, device_id=partner, device_id_type=MESH)
    pl.semaphore_signal(bar, inc=1, device_id=previous, device_id_type=MESH)

    expert = iota((256, NB), 1)
    one0 = (ids[:, 0:1] == expert).astype(F32)
    one1 = (ids[:, 1:2] == expert).astype(F32)
    lower = (iota((256, 256), 0) > iota((256, 256), 1)).astype(BF16)
    place = dot(lower, (one0 + one1).astype(BF16)) + 1.0

    def slot_maps(marks):
        held = (place * marks).astype(BF16)

        def spread(width, per):
            e, col = iota((NB, width), 0), iota((NB, width), 1) // per
            dz = group_dz(col // YN)
            hit = ((e // YN - z - dz + 2 * ZN) & (ZN - 1)) + ((lax.rem(e, YN) - y - lax.rem(col, YN) + 2 * YN) & (YN - 1))
            return dot(held, (hit == 0).astype(BF16))

        return spread(NB * 16, 16), spread(NB * 8, 8)

    slot_main = (lax.rem(iota((256, NB * 16), 1), 16) + 1).astype(F32)
    over_col = iota((256, NB * 8), 1)
    slot_over = (lax.rem(over_col // 4, 2) + 17).astype(F32)
    over_k = lax.rem(over_col, 4)

    loads[0].wait()

    def norm2(i, carry):
        rows = pl.ds(pl.multiple_of(i * 64, 64), 64)
        v = x2[rows, :].astype(F32)
        inv = lax.rsqrt(jnp.mean(v * v, axis=-1, keepdims=True) + EPS)
        cols = pl.ds(pl.multiple_of(t * 512, 512), 512)
        xq[rows, :] = (x2[rows, cols].astype(F32) * inv * g2[:, cols].astype(F32)).astype(BF16)
        return carry

    lax.fori_loop(0, 4, norm2, 0)
    in_main, in_over = slot_maps(one0 + one1)
    pick_main = (in_main == slot_main).astype(BF16)
    xv = xq[...]
    rows_main = dot_t(pick_main, xv)
    rows_over = jnp.zeros((NB * 8, 128), F32)
    for k in range(4):
        s[:, 16 * k : 16 * k + 16, :] = rows_main[:, 128 * k : 128 * k + 128].reshape(NB, 16, 128).astype(BF16)
        pick = jnp.logical_and(in_over == slot_over, over_k == k).astype(BF16)
        rows_over = rows_over + dot_t(pick, xv[:, 128 * k : 128 * k + 128])
    s[:, 64:72, :] = rows_over.reshape(NB, 8, 128).astype(BF16)
    r[0, 0] = s[0]

    pl.semaphore_wait(bar, NB - 1 + 3 + 2)

    def dispatch(b, carry):
        remote(
            s.at[b], r.at[0, b], a_s.at[b], a_r.at[b // YN], at(group_dz(b // YN), lax.rem(b, YN))
        ).start()
        return carry

    lax.fori_loop(1, NB, dispatch, 0)

    swaps = [
        remote(a, b, ws_s.at[i], ws_r.at[i], partner)
        for i, (a, b) in enumerate([(wg_h.at[0], wg2), (wu_h.at[0], wu2), (wd_h.at[0], wd2)])
    ]
    for copy in swaps:
        copy.start()

    half_rows = pl.ds(pl.multiple_of(c * 128, 128), 128)
    outward = []
    for dx in (1, 2, 3):
        cols = pl.ds(pl.multiple_of(lax.rem(t + dx, XN) * 512, 512), 512)
        outward.append(
            remote(pout_h.at[half_rows, cols], wo.at[dx, half_rows], wo_s.at[dx], wo_r.at[dx], along(dx))
        )
    for copy in outward:
        copy.start()
    own_out = pltpu.make_async_copy(
        pout_h.at[:, pl.ds(pl.multiple_of(t * 512, 512), 512)], wo.at[0], sem_in.at[6]
    )
    own_out.start()

    def gather(g):
        rows = pl.ds(pl.multiple_of(g * YN, YN), YN)
        return [remote(r.at[0, rows], r.at[dx, rows], g_s.at[dx, g], g_r.at[dx, g], along(dx)) for dx in (1, 3, 2)]

    def first_arrived():
        remote(s.at[pl.ds(1, 3)], r.at[0, pl.ds(1, 3)], a_s.at[0], a_r.at[0], partner).wait_recv()

    def arrived(g):
        rows = pl.ds(pl.multiple_of(g * YN, YN), YN)
        remote(s.at[rows], r.at[0, rows], a_s.at[0], a_r.at[g], partner).wait_recv()

    loads[1].wait()
    loads[2].wait()

    def norm1(i, carry):
        rows = pl.ds(pl.multiple_of(i * 64, 64), 64)
        v = x1[rows, :].astype(F32)
        inv = lax.rsqrt(jnp.mean(v * v, axis=-1, keepdims=True) + EPS)
        n1[rows, :] = (v * inv * g1[...].astype(F32)).astype(BF16)
        return carry

    lax.fori_loop(0, 8, norm1, 0)
    first_arrived()
    for copy in gather(0):
        copy.start()

    def inward(i, carry):
        rows = pl.ds(pl.multiple_of(i * 256, 256), 256)
        pl_in[rows, :] = dot(n1[rows, :], pin[...]).astype(BF16)
        return carry

    lax.fori_loop(0, 2, inward, 0)
    tail[...] = pl_in[496:512, :]
    halo_copy = remote(tail, halo, h_s, h_r, following)
    halo_copy.start()

    def pass_on(g, carry):
        arrived(g)
        for copy in gather(g):
            copy.start()
        return carry

    lax.fori_loop(1, 4, pass_on, 0)
    halo_copy.wait_recv()
    ext[0:16, :] = jnp.where(ep == 0, 0.0, halo[...].astype(F32))
    ext[16:528, :] = pl_in[...].astype(F32)
    window = jnp.left_shift(jnp.int32(2), t)
    reach = ext[...]
    total = jnp.zeros((528, 256), F32)
    for i in range(4):
        reach = reach + pltpu.roll(reach, 1 << i, 0)
        total = jnp.where(t == i, reach, total)
    count = jnp.minimum(ep * 512 + iota((512, 1), 0) + 1, window).astype(F32)
    mixed = (total[16:528, :] / count - ext[16:528, :]).astype(BF16)
    plx[0] = (dot(mixed, pmix[0]) * psc[...].astype(F32)).astype(BF16)
    for copy in outward:
        copy.wait_recv()
    shared = [
        remote(wo.at[dx, half_rows], wo.at[dx, half_rows], wp_s.at[dx], wp_r.at[dx], partner) for dx in (1, 2, 3)
    ]
    for copy in shared:
        copy.start()
    lax.fori_loop(4, NG, pass_on, 0)

    for copy in loads[3:]:
        copy.wait()
    for copy in swaps:
        copy.wait_recv()

    def expand(k):
        m, n = iota((HALF * 2, HALF * 8), 0), iota((HALF * 2, HALF * 8), 1)
        return (n == (m // 2) * 8 + lax.rem(m, 2) * 4 + k).astype(BF16)

    def collapse(k):
        n, m = iota((HALF * 8, HALF * 2), 0), iota((HALF * 8, HALF * 2), 1)
        return (n == (m // 2) * 8 + lax.rem(m, 2) * 4 + k).astype(BF16)

    def chunk(i, carry):
        blocks = pl.ds(pl.multiple_of(i * HALF, HALF), HALF)

        def take(j, carry2):
            for copy in gather(i * 4 + j):
                copy.wait_recv()
            return carry2

        lax.fori_loop(0, 4, take, 0)
        for dx in range(4):
            q = lax.rem(t - dx + XN, XN)
            over = r[dx, blocks, 64:72, :].astype(F32).reshape(HALF * 8, 128).astype(BF16)
            for k in range(4):
                cols = pl.ds(pl.multiple_of(q * 512 + 128 * k, 128), 128)
                lhs[0 : HALF * 16, cols] = r[dx, blocks, 16 * k : 16 * k + 16, :].reshape(HALF * 16, 128)
                lhs[HALF * 16 : HALF * 18, cols] = dot(expand(k), over).astype(BF16)

        def units(n, carry2):
            cols = pl.ds(pl.multiple_of(n * 256, 256), 256)
            for j, (a, b) in enumerate([(wg, wu), (wg2, wu2)]):
                gate, up = dot(lhs[...], a[:, cols]), dot(lhs[...], b[:, cols])
                hid[j, :, cols] = (gate / (1.0 + jnp.exp(-gate)) * up).astype(BF16)
            return carry2

        lax.fori_loop(0, 2, units, 0)
        for dx in (2, 1, 3, 0):
            q = lax.rem(t + dx, XN)
            over = jnp.zeros((HALF * 8, 128), F32)
            for n in range(2):
                cols = pl.ds(pl.multiple_of(q * 512 + 256 * n, 256), 256)
                term = dot(hid[0], wd[:, cols]) + dot(hid[1], wd2[:, cols])
                for m in range(2):
                    k = 2 * n + m
                    part = term[:, 128 * m : 128 * m + 128]
                    tm[dx, blocks, 16 * k : 16 * k + 16, :] = part[0 : HALF * 16].reshape(HALF, 16, 128).astype(BF16)
                    over = over + dot(collapse(k), part[HALF * 16 :].astype(BF16))
            tm[dx, blocks, 64:72, :] = over.reshape(HALF, 8, 128).astype(BF16)
            if dx:

                def give(j, carry2):
                    reduce_copy(i * 4 + j, dx).start()
                    return carry2

                lax.fori_loop(0, 4, give, 0)
        return carry

    def reduce_copy(g, dx):
        rows = pl.ds(pl.multiple_of(g * YN, YN), YN)
        return remote(tm.at[dx, rows], rr.at[dx, rows], t_s.at[dx, g], t_r.at[dx, g], along(dx))

    def back(b):
        return remote(
            fin.at[b], ret.at[b], b_s.at[b], b_r.at[b // YN], at(ZN - group_dz(b // YN), YN - lax.rem(b, YN))
        )

    def summed(g):
        rows = pl.ds(pl.multiple_of(g * YN, YN), YN)
        for dx in (1, 3, 2):
            reduce_copy(g, dx).wait_recv()
        v = tm[0, rows].astype(F32)
        for dx in (1, 2, 3):
            v = v + rr[dx, rows].astype(F32)
        fin[rows] = v.astype(BF16)

    def give_back(g, carry):
        summed(g)

        def one(dy, carry2):
            back(g * YN + dy).start()
            return carry2

        lax.fori_loop(0, YN, one, 0)
        return carry

    lax.fori_loop(0, 2, chunk, 0)

    spread_pooled = [remote(plx.at[0], plx.at[dx], p_s.at[dx], p_r.at[dx], along(dx)) for dx in (1, 3, 2)]
    for copy in spread_pooled:
        copy.start()

    summed(0)
    ret[0] = fin[0]

    def first_back(b, carry):
        back(b).start()
        return carry

    lax.fori_loop(1, YN, first_back, 0)
    lax.fori_loop(1, NG, give_back, 0)

    own_out.wait()
    for copy in shared:
        copy.wait_recv()
    for copy in spread_pooled:
        copy.wait_recv()
    for n in range(2):
        rows = slice(256 * n, 256 * n + 256)
        acc = dot(plx[0, rows, :], wo[0])
        for dx in (1, 2, 3):
            acc = acc + dot(plx[dx, rows, :], wo[dx])
        out1[rows, :] = acc.astype(BF16)

    logit0, logit1 = lg[:, 0:1], lg[:, 1:2]
    maps = [
        (slot_maps(one0), 1.0 / (1.0 + jnp.exp(logit1 - logit0))),
        (slot_maps(one1), 1.0 / (1.0 + jnp.exp(logit0 - logit1))),
    ]
    remote(fin.at[pl.ds(1, 3)], ret.at[pl.ds(1, 3)], b_s.at[0], b_r.at[0], partner).wait_recv()

    def returned(g, carry):
        rows = pl.ds(pl.multiple_of(g * YN, YN), YN)
        remote(fin.at[rows], ret.at[rows], b_s.at[0], b_r.at[g], partner).wait_recv()
        return carry

    lax.fori_loop(1, NG, returned, 0)
    for k in range(4):
        fm[:, 128 * k : 128 * k + 128] = ret[:, 16 * k : 16 * k + 16, :].reshape(NB * 16, 128)
    fo[...] = ret[:, 64:72, :].astype(F32).reshape(NB * 8, 128).astype(BF16)
    picks = []
    for (main, over), share in maps:
        base = dot((main == slot_main).astype(BF16), fm[...])
        picks.append((base, over == slot_over, share))
    for k in range(4):
        acc = jnp.zeros((256, 128), F32)
        for base, over, share in picks:
            extra = dot(jnp.logical_and(over, over_k == k).astype(BF16), fo[...])
            acc = acc + share * (base[:, 128 * k : 128 * k + 128] + extra)
        out2[:, 128 * k : 128 * k + 128] = acc.astype(BF16)

    def sent_blocks(b, carry):
        remote(s.at[b], r.at[0, b], a_s.at[b], a_r.at[0], partner).wait_send()
        back(b).wait_send()
        return carry

    lax.fori_loop(1, NB, sent_blocks, 0)

    def sent_groups(g, carry):
        for copy in gather(g):
            copy.wait_send()
        for dx in (1, 2, 3):
            reduce_copy(g, dx).wait_send()
        return carry

    lax.fori_loop(0, NG, sent_groups, 0)
    for copy in swaps + outward + shared + spread_pooled + [halo_copy]:
        copy.wait_send()


def local(
    first_input, first_gain, pool_inward, pool_mixing, pool_scale, pool_outward,
    second_input, second_gain, route_ids, route_logits, expert_gate, expert_up, expert_down,
):
    vmem = pl.BlockSpec(memory_space=pltpu.VMEM)
    far = pl.BlockSpec(memory_space=pl.ANY)
    dma = pltpu.SemaphoreType.DMA
    m = HALF * 18
    return pl.pallas_call(
        kernel,
        name="mixer_experts",
        out_shape=(jax.ShapeDtypeStruct((512, 512), BF16), jax.ShapeDtypeStruct((256, 512), BF16)),
        in_specs=[far, vmem, far, vmem, vmem, far, far, vmem, vmem, vmem, far, far, far],
        out_specs=(vmem, vmem),
        scratch_shapes=[
            pltpu.VMEM((512, 2048), BF16),
            pltpu.VMEM((2048, 256), BF16),
            pltpu.VMEM((256, 2048), BF16),
            pltpu.VMEM((2048, 512), BF16),
            pltpu.VMEM((2048, 512), BF16),
            pltpu.VMEM((512, 2048), BF16),
            pltpu.VMEM((2048, 512), BF16),
            pltpu.VMEM((2048, 512), BF16),
            pltpu.VMEM((512, 2048), BF16),
            pltpu.VMEM((512, 2048), BF16),
            pltpu.VMEM((512, 256), BF16),
            pltpu.VMEM((528, 256), F32),
            pltpu.VMEM((16, 256), BF16),
            pltpu.VMEM((16, 256), BF16),
            pltpu.VMEM((4, 512, 256), BF16),
            pltpu.VMEM((4, 256, 512), BF16),
            pltpu.VMEM((256, 512), BF16),
            pltpu.VMEM((NB, 72, 128), BF16),
            pltpu.VMEM((4, NB, 72, 128), BF16),
            pltpu.VMEM((m, 2048), BF16),
            pltpu.VMEM((2, m, 512), BF16),
            pltpu.VMEM((4, NB, 72, 128), BF16),
            pltpu.VMEM((4, NB, 72, 128), BF16),
            pltpu.VMEM((NB, 72, 128), BF16),
            pltpu.VMEM((NB, 72, 128), BF16),
            pltpu.VMEM((NB * 16, 512), BF16),
            pltpu.VMEM((NB * 8, 128), BF16),
            dma((7,)),
            dma((3,)), dma((3,)),
            dma((NB,)), dma((NG,)),
            dma((4, NG)), dma((4, NG)),
            dma((4, NG)), dma((4, NG)),
            dma((NB,)), dma((NG,)),
            dma, dma,
            dma((4,)), dma((4,)),
            dma((4,)), dma((4,)),
            dma((4,)), dma((4,)),
        ],
        compiler_params=pltpu.CompilerParams(
            collective_id=0, has_side_effects=True, vmem_limit_bytes=60 * 1024 * 1024
        ),
    )(
        first_input, first_gain.reshape(1, -1), pool_inward, pool_mixing, pool_scale.reshape(1, -1), pool_outward,
        second_input, second_gain.reshape(1, -1), route_ids, route_logits, expert_gate, expert_up, expert_down,
    )


def solution(mesh):
    placed = (
        P("ep", None), P(), P(None, "tp"), P("tp", None, None), P("tp"), P("tp", None),
        P("ep", None), P(), P("ep", None), P("ep", None),
        P("ep", None, "tp"), P("ep", None, "tp"), P("ep", "tp", None),
    )
    return jax.shard_map(
        local, mesh=mesh, in_specs=placed, out_specs=(P("ep", "tp"), P("ep", "tp")), check_vma=False
    )
```

```python
import jax
import jax.numpy as jnp
from jax import lax
from jax.experimental import pallas as pl
from jax.experimental.pallas import tpu as pltpu
from jax.sharding import PartitionSpec as P

MESH = pl.DeviceIdType.MESH
F32, BF16 = jnp.float32, jnp.bfloat16
EPS = 1e-06
ZN, YN, XN = 8, 4, 4
NB = ZN * YN
NG = ZN
EP = NB * 2
HALF = NB // 2
NR = 3
SELF = NB - YN


def dot(a, b):
    return jnp.dot(a, b, preferred_element_type=F32)


def dot_t(a, b):
    return lax.dot_general(a, b, (((0,), (0,)), ((), ())), preferred_element_type=F32)


def iota(shape, dim):
    return lax.broadcasted_iota(jnp.int32, shape, dim)


def group_dz(g):
    return jnp.where((g & 1) == 1, (7 - g) >> 1, 4 + (g >> 1))


def kernel(
    x1_h, g1, pin_h, pmix, psc, pout_h, x2_h, g2, ids, lg, wg_h, wu_h, wd_h,
    out1, out2,
    x1, pin, x2, wg, wu, wd, wg2, wu2, wd2,
    n1, pl_in, ext, halo, tail, plx, wo, xq,
    s, s2, r, lhs, hid, tm, rr, rv, fin, ret, fm, fo, o1, o2,
    sem_in, ws_s, ws_r, a_s, a_r, a2_s, a2_r, g_s, g_r, y_s, y_r, v_s, v_r, d_s, d_r,
    b_s, b_r, h_s, h_r, wo_s, wo_r, wy_s, wy_r, wp_s, wp_r, p_s, p_r, p2_s, p2_r,
):
    ep, t = lax.axis_index("ep"), lax.axis_index("tp")
    c = lax.rem(ep, 2)
    chip = ep // 2
    y, z = lax.rem(chip, YN), chip // YN

    def at(dz, dy, dc=0):
        z2, y2, c2 = lax.rem(z + dz + ZN, ZN), lax.rem(y + dy + YN, YN), lax.rem(c + dc, 2)
        return ((z2 * YN + y2) * 2 + c2, t)

    def along(dx):
        return (ep, lax.rem(t + dx, XN))

    def quarter(dx):
        return lax.rem(t + dx + XN, XN)

    partner = at(0, 0, 1)
    following = (lax.rem(ep + 1, EP), t)
    previous = (lax.rem(ep + EP - 1, EP), t)

    def remote(src, dst, ss, rs, device):
        return pltpu.make_async_remote_copy(
            src_ref=src, dst_ref=dst, send_sem=ss, recv_sem=rs, device_id=device, device_id_type=MESH
        )

    def blocks_of(g, first=0, count=YN):
        return pl.ds(g * YN + first, count)

    loads = [
        pltpu.make_async_copy(a, b, sem_in.at[i])
        for i, (a, b) in enumerate(
            [(x2_h, x2), (x1_h, x1), (pin_h, pin), (wg_h.at[0], wg), (wu_h.at[0], wu), (wd_h.at[0], wd)]
        )
    ]
    for copy in loads:
        copy.start()

    bar = pltpu.get_barrier_semaphore()

    def greet(b, carry):
        pl.semaphore_signal(bar, inc=1, device_id=at(group_dz(b // YN), lax.rem(b, YN)), device_id_type=MESH)
        return carry

    lax.fori_loop(0, SELF, greet, 0)
    lax.fori_loop(SELF + 1, NB, greet, 0)
    for dx in (1, 2, 3):
        pl.semaphore_signal(bar, inc=1, device_id=along(dx), device_id_type=MESH)
    pl.semaphore_signal(bar, inc=1, device_id=partner, device_id_type=MESH)
    pl.semaphore_signal(bar, inc=1, device_id=previous, device_id_type=MESH)

    expert = iota((NB, 256), 0)
    one0 = (ids[0:1, :] == expert).astype(F32)
    one1 = (ids[1:2, :] == expert).astype(F32)
    earlier = (iota((256, 256), 0) < iota((256, 256), 1)).astype(BF16)
    place = dot((one0 + one1).astype(BF16), earlier) + 1.0

    def slot_maps(marks):
        held = (place * marks).astype(BF16)

        def spread(width, per):
            e, col = iota((NB, width), 0), iota((NB, width), 1) // per
            dz = group_dz(col // YN)
            hit = ((e // YN - z - dz + 2 * ZN) & (ZN - 1)) + ((lax.rem(e, YN) - y - lax.rem(col, YN) + 2 * YN) & (YN - 1))
            return dot_t(held, (hit == 0).astype(BF16))

        return spread(NB * 16, 16), spread(NB * 8, 8)

    slot_main = (lax.rem(iota((256, NB * 16), 1), 16) + 1).astype(F32)
    over_col = iota((256, NB * 8), 1)
    slot_over = (lax.rem(over_col // 4, 2) + 17).astype(F32)
    over_k = lax.rem(over_col, 4)

    loads[0].wait()

    def norm2(i, carry):
        rows = pl.ds(pl.multiple_of(i * 64, 64), 64)
        v = x2[rows, :].astype(F32)
        inv = lax.rsqrt(jnp.mean(v * v, axis=-1, keepdims=True) + EPS)
        for j, dx in enumerate((0, 2)):
            cols = pl.ds(pl.multiple_of(quarter(dx) * 512, 512), 512)
            xq[j, rows, :] = (x2[rows, cols].astype(F32) * inv * g2[cols].astype(F32)).astype(BF16)
        return carry

    lax.fori_loop(0, 4, norm2, 0)
    in_main, in_over = slot_maps(one0 + one1)
    pick_main = (in_main == slot_main).astype(BF16)
    picks_over = [jnp.logical_and(in_over == slot_over, over_k == k).astype(BF16) for k in range(4)]
    for j, buf, skip in ((0, s, 0), (1, s2, NR * YN)):
        xv = xq[j]
        count = NB - skip
        rows_main = dot_t(pick_main[:, skip * 16 :], xv)
        rows_over = jnp.zeros((count * 8, 128), F32)
        for k in range(4):
            lanes = slice(128 * k, 128 * k + 128)
            buf[:, 16 * k : 16 * k + 16, :] = rows_main[:, lanes].reshape(count, 16, 128).astype(BF16)
            rows_over = rows_over + dot_t(picks_over[k][:, skip * 8 :], xv[:, lanes])
        buf[:, 64:72, :] = rows_over.reshape(count, 8, 128).astype(BF16)
        r[2 * j, SELF] = buf[SELF - skip]

    loads[1].wait()
    loads[2].wait()

    def normed1(rows):
        v = x1[rows, :].astype(F32)
        inv = lax.rsqrt(jnp.mean(v * v, axis=-1, keepdims=True) + EPS)
        return (v * inv * g1[...].astype(F32)).astype(BF16)

    tail[...] = dot(normed1(pl.ds(496, 16)), pin[...]).astype(BF16)
    halo_copy = remote(tail, halo, h_s, h_r, following)

    pl.semaphore_wait(bar, NB - 1 + 3 + 2)

    halo_copy.start()

    def toward(b):
        return at(group_dz(b // YN), lax.rem(b, YN))

    def dispatch(b, carry):
        remote(s.at[b], r.at[0, b], a_s, a_r.at[b // YN], toward(b)).start()
        return carry

    def dispatch2(b, carry):
        remote(s2.at[b - NR * YN], r.at[2, b], a2_s, a2_r.at[b // HALF], toward(b)).start()
        return carry

    lax.fori_loop(0, HALF, dispatch, 0)
    lax.fori_loop(NR * YN, HALF, dispatch2, 0)
    for send in (dispatch, dispatch2):
        lax.fori_loop(HALF, SELF, send, 0)
        lax.fori_loop(SELF + 1, NB, send, 0)

    swaps = [
        remote(a, b, ws_s.at[i], ws_r.at[i], partner)
        for i, (a, b) in enumerate([(wg_h.at[0], wg2), (wu_h.at[0], wu2), (wd_h.at[0], wd2)])
    ]
    for copy in swaps:
        copy.start()

    half_rows = pl.ds(pl.multiple_of(c * 128, 128), 128)
    piece = pl.ds(pl.multiple_of(c * 128 + y * 32, 32), 32)
    outward = []
    for dx in (1, 2, 3):
        cols = pl.ds(pl.multiple_of(quarter(dx) * 512, 512), 512)
        outward.append(remote(pout_h.at[piece, cols], wo.at[dx, piece], wo_s, wo_r, along(dx)))
    for copy in outward:
        copy.start()
    along_y = [
        remote(wo.at[pl.ds(1, 3), piece], wo.at[pl.ds(1, 3), piece], wy_s, wy_r, at(0, dy)) for dy in (1, 2, 3)
    ]
    shared = remote(wo.at[pl.ds(1, 3), half_rows], wo.at[pl.ds(1, 3), half_rows], wp_s, wp_r, partner)
    own_out = pltpu.make_async_copy(
        pout_h.at[:, pl.ds(pl.multiple_of(t * 512, 512), 512)], wo.at[0], sem_in.at[6]
    )
    own_out.start()

    def landed(ref, sem):
        remote(ref, ref, a_s, sem, partner).wait_recv()

    def left(ref, sem):
        remote(ref, ref, sem, a_r.at[0], partner).wait_send()

    def gather(g, dx):
        rows = blocks_of(g)
        arrival = g_r.at[dx // 2 * NR + g if g < NR else 2 * NR + g // 4]
        return remote(r.at[0, rows], r.at[dx, rows], g_s, arrival, along(dx))

    def relay(g, dx):
        rows = blocks_of(g, dx - 1, 2)
        return remote(r.at[dx, rows], r.at[2, rows], y_s, y_r, along(dx))

    def arrived(g):
        landed(s.at[pl.ds(0, 3 if g == NG - 1 else YN)], a_r.at[g])

    def pass_on(g):
        arrived(g)
        for dx in (1, 3):
            gather(g, dx).start()

    def relay_on(g):
        for dx in (1, 3):
            gather(g, dx).wait_recv()
            relay(g, dx).start()

    def norm1(i, carry):
        rows = pl.ds(pl.multiple_of(i * 64, 64), 64)
        n1[rows, :] = normed1(rows)
        return carry

    lax.fori_loop(0, 8, norm1, 0)
    def inward(i, carry):
        rows = pl.ds(pl.multiple_of(i * 256, 256), 256)
        pl_in[rows, :] = dot(n1[rows, :], pin[...]).astype(BF16)
        return carry

    lax.fori_loop(0, 2, inward, 0)

    halo_copy.wait_recv()
    ext[0:16, :] = jnp.where(ep == 0, 0.0, halo[...].astype(F32))
    ext[16:528, :] = pl_in[...].astype(F32)
    window = jnp.left_shift(jnp.int32(2), t)
    reach = ext[...]
    total = jnp.zeros((528, 256), F32)
    for i in range(4):
        reach = reach + pltpu.roll(reach, 1 << i, 0)
        total = jnp.where(t == i, reach, total)
    count = jnp.minimum(ep * 512 + iota((512, 1), 0) + 1, window).astype(F32)
    mixed = (total[16:528, :] / count - ext[16:528, :]).astype(BF16)
    plx[0] = (dot(mixed, pmix[0]) * psc[...].astype(F32)).astype(BF16)
    def pooled(dx):
        return remote(plx.at[0], plx.at[dx], p_s, p_r.at[dx // 2], along(dx))

    def pooled_on(dx):
        rows = pl.ds(128 * (dx - 1), 256)
        return remote(plx.at[dx, rows], plx.at[2, rows], p2_s, p2_r, along(dx))

    for dx in (1, 3):
        pooled(dx).start()

    pass_on(0)
    pass_on(1)
    relay_on(0)
    pass_on(2)
    relay_on(1)
    pass_on(3)
    relay_on(2)
    for dx in (1, 3):
        pooled(dx).wait_recv()
        pooled_on(dx).start()
    landed(wo.at[pl.ds(1, 3), piece], wo_r)
    for copy in along_y:
        copy.start()

    def expand(k):
        m, n = iota((HALF * 2, HALF * 8), 0), iota((HALF * 2, HALF * 8), 1)
        return (n == (m // 2) * 8 + lax.rem(m, 2) * 4 + k).astype(BF16)

    def collapse(k):
        n, m = iota((HALF * 8, HALF * 2), 0), iota((HALF * 8, HALF * 2), 1)
        return (n == (m // 2) * 8 + lax.rem(m, 2) * 4 + k).astype(BF16)

    def rows_in(i):
        blocks = pl.ds(i * HALF, HALF)
        for dx in range(4):
            q = quarter(-dx)
            over = r[dx, blocks, 64:72, :].astype(F32).reshape(HALF * 8, 128).astype(BF16)
            for k in range(4):
                cols = pl.ds(pl.multiple_of(q * 512 + 128 * k, 128), 128)
                lhs[0 : HALF * 16, cols] = r[dx, blocks, 16 * k : 16 * k + 16, :].reshape(HALF * 16, 128)
                lhs[HALF * 16 : HALF * 18, cols] = dot(expand(k), over).astype(BF16)

    def units(n, carry):
        cols = pl.ds(pl.multiple_of(n * 256, 256), 256)
        for j, (a, b) in enumerate([(wg, wu), (wg2, wu2)]):
            gate, up = dot(lhs[...], a[:, cols]), dot(lhs[...], b[:, cols])
            hid[j, :, cols] = (gate / (1.0 + jnp.exp(-gate)) * up).astype(BF16)
        return carry

    def down(i, dx):
        blocks = pl.ds(i * HALF, HALF)
        over = jnp.zeros((HALF * 8, 128), F32)
        for n in range(2):
            cols = pl.ds(pl.multiple_of(quarter(dx) * 512 + 256 * n, 256), 256)
            term = dot(hid[0], wd[:, cols]) + dot(hid[1], wd2[:, cols])
            for m in range(2):
                k = 2 * n + m
                part = term[:, 128 * m : 128 * m + 128]
                tm[dx, blocks, 16 * k : 16 * k + 16, :] = part[0 : HALF * 16].reshape(HALF, 16, 128).astype(BF16)
                over = over + dot(collapse(k), part[HALF * 16 :].astype(BF16))
        tm[dx, blocks, 64:72, :] = over.reshape(HALF, 8, 128).astype(BF16)

    def by_way(j, dx):
        rows = blocks_of(2 * j + dx // 2)
        return remote(tm.at[2, rows], rv.at[rows], v_s, v_r.at[dx // 2, j], along(dx))

    def direct(j, dx):
        g = 2 * j + 1 - dx // 2
        rows = blocks_of(g)
        return remote(tm.at[dx, rows], rr.at[dx // 2, rows], d_s, d_r.at[g], along(dx))

    def joined(j, dx):
        g = 2 * j + dx // 2
        rows = blocks_of(g)
        return remote(tm.at[dx, rows], rr.at[dx // 2, rows], d_s, d_r.at[g], along(dx))

    def each(first, last, action):
        def body(g, carry):
            action(g)
            return carry

        lax.fori_loop(first, last, body, 0)

    def start_by_way(j):
        for dx in (1, 3):
            by_way(j, dx).start()

    def join(j):
        for dx in (1, 3):
            by_way(j, dx).wait_recv()
            rows = blocks_of(2 * j + dx // 2)
            tm[dx, rows] = (tm[dx, rows].astype(F32) + rv[rows].astype(F32)).astype(BF16)
            joined(j, dx).start()

    def back(b):
        return remote(fin.at[b], ret.at[b], b_s, b_r, at(ZN - group_dz(b // YN), YN - lax.rem(b, YN)))

    def summed(g):
        rows = blocks_of(g)
        landed(s.at[pl.ds(0, 2 * YN)], d_r.at[g])
        v = tm[0, rows].astype(F32) + rr[0, rows].astype(F32) + rr[1, rows].astype(F32)
        fin[rows] = v.astype(BF16)

    def give_back(g):
        summed(g)
        for dy in range(YN):
            back(g * YN + dy).start()

    landed(s.at[pl.ds(0, NR * YN)], y_r)
    landed(s.at[pl.ds(0, 2 * YN)], g_r.at[2 * NR])
    landed(s.at[pl.ds(0, YN)], a2_r.at[0])
    for copy in loads[3:]:
        copy.wait()
    for copy in swaps:
        copy.wait_recv()
    pass_on(4)
    rows_in(0)
    pass_on(5)
    lax.fori_loop(0, 2, units, 0)
    pass_on(6)
    pass_on(7)
    down(0, 2)
    each(0, 2, start_by_way)
    for dx in (1, 3):
        down(0, dx)
        each(0, 2, lambda j: direct(j, dx).start())
    down(0, 0)
    landed(s, g_r.at[2 * NR + 1])
    landed(s.at[pl.ds(0, HALF - 1)], a2_r.at[1])
    rows_in(1)
    lax.fori_loop(0, 2, units, 0)
    landed(wo.at[pl.ds(1, 3), pl.ds(0, 96)], wy_r)
    shared.start()
    each(0, 2, join)

    down(1, 2)
    each(2, 4, start_by_way)
    for dx in (1, 3):
        down(1, dx)
        each(2, 4, lambda j: direct(j, dx).start())
    each(0, 4, give_back)
    down(1, 0)
    each(2, 4, join)
    each(4, NG - 1, give_back)
    summed(NG - 1)
    ret[SELF] = fin[SELF]
    for dy in range(1, YN):
        back(SELF + dy).start()

    row0 = iota((8, 256), 0) == 0
    gap = lg[1:2, :] - lg[0:1, :]
    shares = jnp.where(row0, 1.0 / (1.0 + jnp.exp(gap)), 1.0 / (1.0 + jnp.exp(-gap))).T
    maps = [(slot_maps(one0), shares[:, 0:1]), (slot_maps(one1), shares[:, 1:2])]
    own_out.wait()
    shared.wait_recv()
    landed(plx.at[0], p2_r)
    for n in range(2):
        rows = slice(256 * n, 256 * n + 256)
        acc = dot(plx[0, rows, :], wo[0])
        for dx in (1, 2, 3):
            acc = acc + dot(plx[dx, rows, :], wo[dx])
        o1[rows, :] = acc.astype(BF16)
    write1 = pltpu.make_async_copy(o1, out1, sem_in.at[7])
    write1.start()

    landed(s.at[pl.ds(0, NB - 1)], b_r)
    for k in range(4):
        fm[:, 128 * k : 128 * k + 128] = ret[:, 16 * k : 16 * k + 16, :].reshape(NB * 16, 128)
    fo[...] = ret[:, 64:72, :].astype(F32).reshape(NB * 8, 128).astype(BF16)
    picks = []
    for (main, over), share in maps:
        base = dot((main == slot_main).astype(BF16), fm[...])
        picks.append((base, over == slot_over, share))
    for k in range(4):
        acc = jnp.zeros((256, 128), F32)
        for base, over, share in picks:
            extra = dot(jnp.logical_and(over, over_k == k).astype(BF16), fo[...])
            acc = acc + share * (base[:, 128 * k : 128 * k + 128] + extra)
        o2[:, 128 * k : 128 * k + 128] = acc.astype(BF16)
    write2 = pltpu.make_async_copy(o2, out2, sem_in.at[8])
    write2.start()

    left(s.at[pl.ds(0, NB - 1)], a_s)
    left(s.at[pl.ds(0, NB - NR * YN - 1)], a2_s)
    left(r.at[pl.ds(0, 2)], g_s)
    left(s.at[pl.ds(0, NR * YN)], y_s)
    left(s, v_s)
    left(r.at[pl.ds(0, 2)], d_s)
    left(s.at[pl.ds(0, NB - 1)], b_s)
    left(plx.at[pl.ds(0, 2)], p_s)
    left(plx.at[0], p2_s)
    left(wo.at[pl.ds(1, 3), piece], wo_s)
    left(wo.at[pl.ds(1, 3), pl.ds(0, 96)], wy_s)
    for copy in swaps + [shared, halo_copy]:
        copy.wait_send()
    write1.wait()
    write2.wait()


def local(
    first_input, first_gain, pool_inward, pool_mixing, pool_scale, pool_outward,
    second_input, second_gain, route_ids, route_logits, expert_gate, expert_up, expert_down,
):
    vmem = pl.BlockSpec(memory_space=pltpu.VMEM)
    far = pl.BlockSpec(memory_space=pl.ANY)
    dma = pltpu.SemaphoreType.DMA
    m = HALF * 18
    return pl.pallas_call(
        kernel,
        name="mixer_experts",
        out_shape=(jax.ShapeDtypeStruct((512, 512), BF16), jax.ShapeDtypeStruct((256, 512), BF16)),
        in_specs=[far, vmem, far, vmem, vmem, far, far, vmem, vmem, vmem, far, far, far],
        out_specs=(far, far),
        scratch_shapes=[
            pltpu.VMEM((512, 2048), BF16),
            pltpu.VMEM((2048, 256), BF16),
            pltpu.VMEM((256, 2048), BF16),
            pltpu.VMEM((2048, 512), BF16),
            pltpu.VMEM((2048, 512), BF16),
            pltpu.VMEM((512, 2048), BF16),
            pltpu.VMEM((2048, 512), BF16),
            pltpu.VMEM((2048, 512), BF16),
            pltpu.VMEM((512, 2048), BF16),
            pltpu.VMEM((512, 2048), BF16),
            pltpu.VMEM((512, 256), BF16),
            pltpu.VMEM((528, 256), F32),
            pltpu.VMEM((16, 256), BF16),
            pltpu.VMEM((16, 256), BF16),
            pltpu.VMEM((4, 512, 256), BF16),
            pltpu.VMEM((4, 256, 512), BF16),
            pltpu.VMEM((2, 256, 512), BF16),
            pltpu.VMEM((NB, 72, 128), BF16),
            pltpu.VMEM((NB - NR * YN, 72, 128), BF16),
            pltpu.VMEM((4, NB, 72, 128), BF16),
            pltpu.VMEM((m, 2048), BF16),
            pltpu.VMEM((2, m, 512), BF16),
            pltpu.VMEM((4, NB, 72, 128), BF16),
            pltpu.VMEM((2, NB, 72, 128), BF16),
            pltpu.VMEM((NB, 72, 128), BF16),
            pltpu.VMEM((NB, 72, 128), BF16),
            pltpu.VMEM((NB, 72, 128), BF16),
            pltpu.VMEM((NB * 16, 512), BF16),
            pltpu.VMEM((NB * 8, 128), BF16),
            pltpu.VMEM((512, 512), BF16),
            pltpu.VMEM((256, 512), BF16),
            dma((9,)),
            dma((3,)), dma((3,)),
            dma, dma((NG,)),
            dma, dma((2,)),
            dma, dma((2 * NR + 2,)),
            dma, dma,
            dma, dma((2, 4)),
            dma, dma((NG,)),
            dma, dma,
            dma, dma,
            dma, dma,
            dma, dma,
            dma, dma,
            dma, dma((2,)),
            dma, dma,
        ],
        compiler_params=pltpu.CompilerParams(
            collective_id=0, has_side_effects=True, vmem_limit_bytes=60 * 1024 * 1024
        ),
    )(
        first_input, first_gain, pool_inward, pool_mixing, pool_scale, pool_outward,
        second_input, second_gain, route_ids.T, route_logits.T, expert_gate, expert_up, expert_down,
    )


def solution(mesh):
    placed = (
        P("ep", None), P(), P(None, "tp"), P("tp", None, None), P("tp"), P("tp", None),
        P("ep", None), P(), P("ep", None), P("ep", None),
        P("ep", None, "tp"), P("ep", None, "tp"), P("ep", "tp", None),
    )
    return jax.shard_map(
        local, mesh=mesh, in_specs=placed, out_specs=(P("ep", "tp"), P("ep", "tp")), check_vma=False
    )
```

```python
import jax
import jax.numpy as jnp
from jax import lax
from jax.experimental import pallas as pl
from jax.experimental.pallas import tpu as pltpu
from jax.sharding import PartitionSpec as P

MESH = pl.DeviceIdType.MESH
F32, BF16 = jnp.float32, jnp.bfloat16
EPS = 1e-06
ZN, YN, XN = 8, 4, 4
NB = ZN * YN
NG = ZN
EP = NB * 2
HALF = NB // 2
ORDER = (3, 5, 4, 0, 2, 6, 1, 7)
NR = 3
SELF = 3 * YN


def dot(a, b):
    return jnp.dot(a, b, preferred_element_type=F32)


def dot_t(a, b):
    return lax.dot_general(a, b, (((0,), (0,)), ((), ())), preferred_element_type=F32)


def iota(shape, dim):
    return lax.broadcasted_iota(jnp.int32, shape, dim)


def group_dz(g):
    dz = jnp.full_like(g, ORDER[0])
    for i in range(1, NG):
        dz = jnp.where(g == i, ORDER[i], dz)
    return dz


def kernel(
    x1_h, g1_h, pin_h, pmix_h, psc_h, pout_h, x2_h, g2_h, ids_h, lg_h, wg_h, wu_h, wd_h,
    out1, out2,
    ids, g2, g1, pmix, psc, lg, x1, pin, x2, wg, wu, wd, wg2, wu2,
    n1, pl_in, ext, halo, tail, plx, wo, xq,
    s, s1, s2, s3, r, lhs, hid, tm, rr, rv, fin, ret, fm, fo,
    sem_in, ws_s, ws_r, a_s, a_r, a2_s, n_s, n_r, g_s, g_r, y_s, y_r, v_s, v_r, d_s, d_r,
    b_s, b_r, h_s, h_r, wo_s, wo_r, wy_s, wy_r, wp_s, wp_r, p_s, p_r, p2_s, p2_r,
):
    ep, t = lax.axis_index("ep"), lax.axis_index("tp")
    c = lax.rem(ep, 2)
    chip = ep // 2
    y, z = lax.rem(chip, YN), chip // YN

    def at(dz, dy, dc=0):
        z2, y2, c2 = lax.rem(z + dz + ZN, ZN), lax.rem(y + dy + YN, YN), lax.rem(c + dc, 2)
        return ((z2 * YN + y2) * 2 + c2, t)

    def along(dx):
        return (ep, lax.rem(t + dx, XN))

    def quarter(dx):
        return lax.rem(t + dx + XN, XN)

    partner = at(0, 0, 1)
    following = (lax.rem(ep + 1, EP), t)
    previous = (lax.rem(ep + EP - 1, EP), t)

    def remote(src, dst, ss, rs, device):
        return pltpu.make_async_remote_copy(
            src_ref=src, dst_ref=dst, send_sem=ss, recv_sem=rs, device_id=device, device_id_type=MESH
        )

    def blocks_of(g, first=0, count=YN):
        return pl.ds(g * YN + first, count)

    loads = [
        pltpu.make_async_copy(a, b, sem_in.at[i])
        for i, (a, b) in enumerate(
            [(x2_h, x2), (x1_h, x1), (pin_h, pin), (wg_h.at[0], wg), (wu_h.at[0], wu), (wd_h.at[0], wd.at[pl.ds(0, 512)])]
        )
    ]
    small = [
        pltpu.make_async_copy(a, b, sem_in.at[7 + i])
        for i, (a, b) in enumerate([(ids_h, ids), (g2_h, g2), (g1_h, g1), (pmix_h, pmix), (psc_h, psc), (lg_h, lg)])
    ]
    for copy in small + loads:
        copy.start()

    bar = pltpu.get_barrier_semaphore()

    def greet(b, carry):
        pl.semaphore_signal(bar, inc=1, device_id=at(group_dz(b // YN), lax.rem(b, YN)), device_id_type=MESH)
        return carry

    lax.fori_loop(0, SELF, greet, 0)
    lax.fori_loop(SELF + 1, NB, greet, 0)
    for dx in (1, 2, 3):
        pl.semaphore_signal(bar, inc=1, device_id=along(dx), device_id_type=MESH)
    pl.semaphore_signal(bar, inc=1, device_id=partner, device_id_type=MESH)
    pl.semaphore_signal(bar, inc=1, device_id=previous, device_id_type=MESH)

    for copy in small:
        copy.wait()
    expert = iota((NB, 256), 0)
    one0 = (ids[0:1, :] == expert).astype(F32)
    one1 = (ids[1:2, :] == expert).astype(F32)
    earlier = (iota((256, 256), 0) < iota((256, 256), 1)).astype(BF16)
    place = dot((one0 + one1).astype(BF16), earlier) + 1.0

    def slot_maps(marks):
        held = (place * marks).astype(BF16)

        def spread(width, per):
            e, col = iota((NB, width), 0), iota((NB, width), 1) // per
            dz = group_dz(col // YN)
            hit = ((e // YN - z - dz + 2 * ZN) & (ZN - 1)) + ((lax.rem(e, YN) - y - lax.rem(col, YN) + 2 * YN) & (YN - 1))
            return dot_t(held, (hit == 0).astype(BF16))

        return spread(NB * 16, 16), spread(NB * 8, 8)

    slot_main = (lax.rem(iota((256, NB * 16), 1), 16) + 1).astype(F32)
    over_col = iota((256, NB * 8), 1)
    slot_over = (lax.rem(over_col // 4, 2) + 17).astype(F32)
    over_k = lax.rem(over_col, 4)

    loads[0].wait()

    def norm2(i, carry):
        rows = pl.ds(pl.multiple_of(i * 64, 64), 64)
        v = x2[rows, :].astype(F32)
        inv = lax.rsqrt(jnp.mean(v * v, axis=-1, keepdims=True) + EPS)
        for dx in range(4):
            cols = pl.ds(pl.multiple_of(quarter(-dx) * 512, 512), 512)
            xq[dx, rows, :] = (x2[rows, cols].astype(F32) * inv * g2[cols].astype(F32)).astype(BF16)
        return carry

    lax.fori_loop(0, 4, norm2, 0)
    in_main, in_over = slot_maps(one0 + one1)
    pick_main = (in_main == slot_main).astype(BF16)
    picks_over = [jnp.logical_and(in_over == slot_over, over_k == k).astype(BF16) for k in range(4)]

    def fill(buf, dx, skip):
        xv = xq[dx]
        count = NB - skip
        rows_main = dot_t(pick_main[:, skip * 16 :], xv)
        rows_over = jnp.zeros((count * 8, 128), F32)
        for k in range(4):
            lanes = slice(128 * k, 128 * k + 128)
            buf[:, 16 * k : 16 * k + 16, :] = rows_main[:, lanes].reshape(count, 16, 128).astype(BF16)
            rows_over = rows_over + dot_t(picks_over[k][:, skip * 8 :], xv[:, lanes])
        buf[:, 64:72, :] = rows_over.reshape(count, 8, 128).astype(BF16)
        r[dx, SELF] = buf[SELF - skip]

    fill(s, 0, 0)

    loads[1].wait()
    loads[2].wait()

    def normed1(rows):
        v = x1[rows, :].astype(F32)
        inv = lax.rsqrt(jnp.mean(v * v, axis=-1, keepdims=True) + EPS)
        return (v * inv * g1[...].astype(F32)).astype(BF16)

    tail[...] = dot(normed1(pl.ds(496, 16)), pin[...]).astype(BF16)
    halo_copy = remote(tail, halo, h_s, h_r, following)

    pl.semaphore_wait(bar, NB - 1 + 3 + 2)

    halo_copy.start()

    def toward(b):
        return at(group_dz(b // YN), lax.rem(b, YN))

    def send_blocks(buf, dx, skip, g, ss, arrival):
        def body(dy, carry):
            b = g * YN + dy
            remote(buf.at[b - skip], r.at[dx, b], ss, arrival, at(ORDER[g], dy)).start()
            return carry

        lax.fori_loop(1 if ORDER[g] == 0 else 0, YN, body, 0)

    half_rows = pl.ds(pl.multiple_of(c * 128, 128), 128)
    piece = pl.ds(pl.multiple_of(c * 128 + y * 32, 32), 32)
    outward = []
    for dx in (1, 2, 3):
        cols = pl.ds(pl.multiple_of(quarter(dx) * 512, 512), 512)
        outward.append(remote(pout_h.at[piece, cols], wo.at[dx, piece], wo_s, wo_r, along(dx)))
    for copy in outward:
        copy.start()
    along_y = [
        remote(wo.at[pl.ds(1, 3), piece], wo.at[pl.ds(1, 3), piece], wy_s, wy_r, at(0, dy)) for dy in (1, 2, 3)
    ]
    shared = remote(wo.at[pl.ds(1, 3), half_rows], wo.at[pl.ds(1, 3), half_rows], wp_s, wp_r, partner)
    for g in range(NR):
        send_blocks(s, 0, 0, g, a_s, a_r.at[g])
    send_blocks(s, 0, 0, NR, a_s, n_r.at[0])

    swaps = [
        remote(a, b, ws_s.at[i], ws_r.at[i], partner)
        for i, (a, b) in enumerate([(wg_h.at[0], wg2), (wu_h.at[0], wu2), (wd_h.at[0], wd.at[pl.ds(512, 512)])])
    ]
    for copy in swaps:
        copy.start()

    own_out = pltpu.make_async_copy(
        pout_h.at[:, pl.ds(pl.multiple_of(t * 512, 512), 512)], wo.at[0], sem_in.at[6]
    )
    own_out.start()

    def landed(ref, sem):
        remote(ref, ref, a_s, sem, partner).wait_recv()

    def left(ref, sem):
        remote(ref, ref, sem, a_r.at[0], partner).wait_send()

    def gather(g, dx):
        rows = blocks_of(g)
        arrival = g_r.at[2 * g + dx // 2 if g < NR - 1 else g // 4 + 2 * NR - 2]
        return remote(r.at[0, rows], r.at[dx, rows], g_s, arrival, along(dx))

    def relay(g, dx):
        rows = blocks_of(g, dx - 1, 2)
        return remote(r.at[dx, rows], r.at[2, rows], y_s, y_r, along(dx))

    def arrived(g):
        landed(s.at[pl.ds(0, YN)], a_r.at[g])

    def pass_on(g):
        arrived(g)
        for dx in (1, 3, 2) if g == NR - 1 else (1, 3):
            gather(g, dx).start()

    def relay_on(g):
        for dx in (1, 3):
            gather(g, dx).wait_recv()
            relay(g, dx).start()

    def norm1(i, carry):
        rows = pl.ds(pl.multiple_of(i * 64, 64), 64)
        n1[rows, :] = normed1(rows)
        return carry

    lax.fori_loop(0, 8, norm1, 0)
    def inward(i, carry):
        rows = pl.ds(pl.multiple_of(i * 256, 256), 256)
        pl_in[rows, :] = dot(n1[rows, :], pin[...]).astype(BF16)
        return carry

    lax.fori_loop(0, 2, inward, 0)

    halo_copy.wait_recv()
    ext[0:16, :] = jnp.where(ep == 0, 0.0, halo[...].astype(F32))
    ext[16:528, :] = pl_in[...].astype(F32)
    window = jnp.left_shift(jnp.int32(2), t)
    reach = ext[...]
    total = jnp.zeros((528, 256), F32)
    for i in range(4):
        reach = reach + pltpu.roll(reach, 1 << i, 0)
        total = jnp.where(t == i, reach, total)
    count = jnp.minimum(ep * 512 + iota((512, 1), 0) + 1, window).astype(F32)
    mixed = (total[16:528, :] / count - ext[16:528, :]).astype(BF16)
    plx[0] = (dot(mixed, pmix[0]) * psc[...].astype(F32)).astype(BF16)
    def pooled(dx):
        return remote(plx.at[0], plx.at[dx], p_s, p_r.at[dx // 2], along(dx))

    def pooled_on(dx):
        rows = pl.ds(128 * (dx - 1), 256)
        return remote(plx.at[dx, rows], plx.at[2, rows], p2_s, p2_r, along(dx))

    for dx in (1, 3):
        pooled(dx).start()

    for dx in (1, 2, 3):
        fill((s1, s2, s3)[dx - 1], dx, NR * YN)
    for g in (3, 4, 5, 6, 7):
        whole = ORDER[g] in (0, 1, 7)
        for buf, dx, ss in ((s, 0, a_s), (s2, 2, a2_s), (s1, 1, n_s), (s3, 3, n_s)):
            if dx == 0 and g > NR:
                send_blocks(s, 0, 0, g, a_s, n_r.at[1] if whole else a_r.at[g])
            elif dx == 2 or (dx and whole):
                send_blocks(buf, dx, NR * YN, g, ss, n_r.at[g // 4])
    pass_on(0)
    pass_on(1)
    pass_on(2)
    relay_on(0)
    relay_on(1)
    pass_on(4)
    pass_on(5)
    landed(wo.at[pl.ds(1, 3), piece], wo_r)
    for copy in along_y:
        copy.start()

    def expand(k):
        m, n = iota((HALF * 2, HALF * 8), 0), iota((HALF * 2, HALF * 8), 1)
        return (n == (m // 2) * 8 + lax.rem(m, 2) * 4 + k).astype(BF16)

    def rows_in(i):
        blocks = pl.ds(i * HALF, HALF)
        for dx in range(4):
            q = quarter(-dx)
            over = r[dx, blocks, 64:72, :].astype(F32).reshape(HALF * 8, 128).astype(BF16)
            for k in range(4):
                cols = pl.ds(pl.multiple_of(q * 512 + 128 * k, 128), 128)
                lhs[0 : HALF * 16, cols] = r[dx, blocks, 16 * k : 16 * k + 16, :].reshape(HALF * 16, 128)
                lhs[HALF * 16 : HALF * 18, cols] = dot(expand(k), over).astype(BF16)

    def units(n, carry):
        cols = pl.ds(n * 256, 256) if isinstance(n, int) else pl.ds(pl.multiple_of(n * 256, 256), 256)
        for j, (a, b) in enumerate([(wg, wu), (wg2, wu2)]):
            gate, up = dot(lhs[...], a[:, cols]), dot(lhs[...], b[:, cols])
            hid[:, pl.ds(512 * j + n * 256, 256) if isinstance(n, int) else pl.ds(pl.multiple_of(512 * j + n * 256, 256), 256)] = (gate / (1.0 + jnp.exp(-gate)) * up).astype(BF16)
        return carry

    def down(i, dx):
        blocks = pl.ds(i * HALF, HALF)
        cols = pl.ds(pl.multiple_of(quarter(dx) * 512, 512), 512)
        term = dot(hid[...], wd[:, cols])
        n, m = iota((HALF * 8, HALF * 2), 0), iota((HALF * 8, HALF * 2), 1)
        spread = dot((n // 4 == m).astype(BF16), term[HALF * 16 :].astype(BF16))
        lane_group = lax.rem(iota((HALF * 8, 128), 0), 4)
        over = spread[:, 0:128]
        for k in range(4):
            part = term[0 : HALF * 16, 128 * k : 128 * k + 128]
            tm[dx, blocks, 16 * k : 16 * k + 16, :] = part.reshape(HALF, 16, 128).astype(BF16)
            if k:
                over = jnp.where(lane_group == k, spread[:, 128 * k : 128 * k + 128], over)
        tm[dx, blocks, 64:72, :] = over.reshape(HALF, 8, 128).astype(BF16)

    def by_way(j, dx):
        rows = blocks_of(2 * j + dx // 2)
        return remote(tm.at[2, rows], rv.at[rows], v_s, v_r.at[dx // 2, j], along(dx))

    def direct(j, dx):
        g = 2 * j + 1 - dx // 2
        rows = blocks_of(g)
        return remote(tm.at[dx, rows], rr.at[dx // 2, rows], d_s, d_r.at[g], along(dx))

    def joined(j, dx):
        g = 2 * j + dx // 2
        rows = blocks_of(g)
        return remote(tm.at[dx, rows], rr.at[dx // 2, rows], d_s, d_r.at[g], along(dx))

    def each(first, last, action):
        def body(g, carry):
            action(g)
            return carry

        lax.fori_loop(first, last, body, 0)

    def start_by_way(j):
        for dx in (1, 3):
            by_way(j, dx).start()

    def join(j):
        for dx in (1, 3):
            by_way(j, dx).wait_recv()
            rows = blocks_of(2 * j + dx // 2)
            tm[dx, rows] = (tm[dx, rows].astype(F32) + rv[rows].astype(F32)).astype(BF16)
            joined(j, dx).start()

    def back(b):
        return remote(fin.at[b], ret.at[b], b_s, b_r, at(ZN - group_dz(b // YN), YN - lax.rem(b, YN)))

    def summed(g):
        rows = blocks_of(g)
        landed(s.at[pl.ds(0, 2 * YN)], d_r.at[g])
        v = tm[0, rows].astype(F32) + rr[0, rows].astype(F32) + rr[1, rows].astype(F32)
        fin[rows] = v.astype(BF16)

    def give_back(g):
        summed(g)
        for dy in range(YN):
            back(g * YN + dy).start()

    landed(s.at[pl.ds(0, (NR - 1) * YN)], y_r)
    landed(s.at[pl.ds(0, NR * YN)], g_r.at[2 * NR - 2])
    landed(s.at[pl.ds(0, NR * YN)], n_r.at[0])
    for copy in loads[3:]:
        copy.wait()
    for copy in swaps:
        copy.wait_recv()
    rows_in(0)
    lax.fori_loop(0, 2, units, 0)
    down(0, 2)
    each(0, 2, start_by_way)
    for dx in (1, 3):
        down(0, dx)
        each(0, 2, lambda j: direct(j, dx).start())
    down(0, 0)
    landed(s.at[pl.ds(0, HALF)], g_r.at[2 * NR - 1])
    landed(r.at[pl.ds(0, 2), pl.ds(0, 20)], n_r.at[1])
    rows_in(1)
    units(0, 0)
    landed(wo.at[pl.ds(1, 3), pl.ds(0, 96)], wy_r)
    shared.start()
    each(0, 2, join)

    units(1, 0)
    down(1, 2)
    each(2, 4, start_by_way)
    for dx in (1, 3):
        down(1, dx)
        each(2, 4, lambda j: direct(j, dx).start())
    down(1, 0)
    each(0, NR, give_back)
    summed(NR)
    ret[SELF] = fin[SELF]
    for dy in range(1, YN):
        back(SELF + dy).start()
    each(2, 4, join)
    for dx in (1, 3):
        pooled(dx).wait_recv()
        pooled_on(dx).start()
    each(4, NG, give_back)

    row0 = iota((8, 256), 0) == 0
    gap = lg[1:2, :] - lg[0:1, :]
    shares = jnp.where(row0, 1.0 / (1.0 + jnp.exp(gap)), 1.0 / (1.0 + jnp.exp(-gap))).T
    maps = [(slot_maps(one0), shares[:, 0:1]), (slot_maps(one1), shares[:, 1:2])]
    own_out.wait()
    shared.wait_recv()
    landed(plx.at[0], p2_r)
    for n in range(2):
        rows = slice(256 * n, 256 * n + 256)
        acc = dot(plx[0, rows, :], wo[0])
        for dx in (1, 2, 3):
            acc = acc + dot(plx[dx, rows, :], wo[dx])
        out1[rows, :] = acc.astype(BF16)

    landed(s.at[pl.ds(0, NB - 1)], b_r)
    for k in range(4):
        fm[:, 128 * k : 128 * k + 128] = ret[:, 16 * k : 16 * k + 16, :].reshape(NB * 16, 128)
    fo[...] = ret[:, 64:72, :].astype(F32).reshape(NB * 8, 128).astype(BF16)
    picks = []
    for (main, over), share in maps:
        base = dot((main == slot_main).astype(BF16), fm[...])
        picks.append((base, over == slot_over, share))
    for k in range(4):
        acc = jnp.zeros((256, 128), F32)
        for base, over, share in picks:
            extra = dot(jnp.logical_and(over, over_k == k).astype(BF16), fo[...])
            acc = acc + share * (base[:, 128 * k : 128 * k + 128] + extra)
        out2[:, 128 * k : 128 * k + 128] = acc.astype(BF16)

    left(s.at[pl.ds(0, NB - 1)], a_s)
    left(s.at[pl.ds(0, NB - NR * YN - 1)], a2_s)
    left(s.at[pl.ds(0, 22)], n_s)
    left(r.at[pl.ds(0, 2), pl.ds(0, 22)], g_s)
    left(s.at[pl.ds(0, (NR - 1) * YN)], y_s)
    left(s, v_s)
    left(r.at[pl.ds(0, 2)], d_s)
    left(s.at[pl.ds(0, NB - 1)], b_s)
    left(plx.at[pl.ds(0, 2)], p_s)
    left(plx.at[0], p2_s)
    left(wo.at[pl.ds(1, 3), piece], wo_s)
    left(wo.at[pl.ds(1, 3), pl.ds(0, 96)], wy_s)
    for copy in swaps + [shared, halo_copy]:
        copy.wait_send()


def local(
    first_input, first_gain, pool_inward, pool_mixing, pool_scale, pool_outward,
    second_input, second_gain, route_ids, route_logits, expert_gate, expert_up, expert_down,
):
    vmem = pl.BlockSpec(memory_space=pltpu.VMEM)
    far = pl.BlockSpec(memory_space=pl.ANY)
    dma = pltpu.SemaphoreType.DMA
    m = HALF * 18
    return pl.pallas_call(
        kernel,
        name="mixer_experts",
        out_shape=(pltpu.VMEM((512, 512), BF16), pltpu.VMEM((256, 512), BF16)),
        in_specs=[far] * 13,
        out_specs=(vmem, vmem),
        scratch_shapes=[
            pltpu.VMEM((2, 256), jnp.int32),
            pltpu.VMEM((2048,), BF16),
            pltpu.VMEM((2048,), BF16),
            pltpu.VMEM((1, 256, 256), BF16),
            pltpu.VMEM((256,), BF16),
            pltpu.VMEM((2, 256), F32),
            pltpu.VMEM((512, 2048), BF16),
            pltpu.VMEM((2048, 256), BF16),
            pltpu.VMEM((256, 2048), BF16),
            pltpu.VMEM((2048, 512), BF16),
            pltpu.VMEM((2048, 512), BF16),
            pltpu.VMEM((1024, 2048), BF16),
            pltpu.VMEM((2048, 512), BF16),
            pltpu.VMEM((2048, 512), BF16),
            pltpu.VMEM((512, 2048), BF16),
            pltpu.VMEM((512, 256), BF16),
            pltpu.VMEM((528, 256), F32),
            pltpu.VMEM((16, 256), BF16),
            pltpu.VMEM((16, 256), BF16),
            pltpu.VMEM((4, 512, 256), BF16),
            pltpu.VMEM((4, 256, 512), BF16),
            pltpu.VMEM((4, 256, 512), BF16),
            pltpu.VMEM((NB, 72, 128), BF16),
            pltpu.VMEM((NB - NR * YN, 72, 128), BF16),
            pltpu.VMEM((NB - NR * YN, 72, 128), BF16),
            pltpu.VMEM((NB - NR * YN, 72, 128), BF16),
            pltpu.VMEM((4, NB, 72, 128), BF16),
            pltpu.VMEM((m, 2048), BF16),
            pltpu.VMEM((m, 1024), BF16),
            pltpu.VMEM((4, NB, 72, 128), BF16),
            pltpu.VMEM((2, NB, 72, 128), BF16),
            pltpu.VMEM((NB, 72, 128), BF16),
            pltpu.VMEM((NB, 72, 128), BF16),
            pltpu.VMEM((NB, 72, 128), BF16),
            pltpu.VMEM((NB * 16, 512), BF16),
            pltpu.VMEM((NB * 8, 128), BF16),
            dma((13,)),
            dma((3,)), dma((3,)),
            dma, dma((6,)),
            dma, dma, dma((2,)),
            dma, dma((2 * NR,)),
            dma, dma,
            dma, dma((2, 4)),
            dma, dma((NG,)),
            dma, dma,
            dma, dma,
            dma, dma,
            dma, dma,
            dma, dma,
            dma, dma((2,)),
            dma, dma,
        ],
        compiler_params=pltpu.CompilerParams(
            collective_id=0, has_side_effects=True, vmem_limit_bytes=64000 * 1024
        ),
    )(
        first_input, first_gain, pool_inward, pool_mixing, pool_scale, pool_outward,
        second_input, second_gain, route_ids.T, route_logits.T, expert_gate, expert_up, expert_down,
    )


def solution(mesh):
    placed = (
        P("ep", None), P(), P(None, "tp"), P("tp", None, None), P("tp"), P("tp", None),
        P("ep", None), P(), P("ep", None), P("ep", None),
        P("ep", None, "tp"), P("ep", None, "tp"), P("ep", "tp", None),
    )
    return jax.shard_map(
        local, mesh=mesh, in_specs=placed, out_specs=(P("ep", "tp"), P("ep", "tp")), check_vma=False
    )
```

```python
import jax
import jax.numpy as jnp
from jax import lax
from jax.experimental import pallas as pl
from jax.experimental.pallas import tpu as pltpu
from jax.sharding import PartitionSpec as P

MESH = pl.DeviceIdType.MESH
F32, BF16 = jnp.float32, jnp.bfloat16
EPS = 1e-06
ZN, YN, XN = 8, 4, 4
NB = ZN * YN
NG = ZN
EP = NB * 2
PAIR = 2 * YN
ORDER = (3, 5, 4, 0, 2, 6, 1, 7)
NR = 3
SELF = 3 * YN


def dot(a, b):
    return jnp.dot(a, b, preferred_element_type=F32)


def dot_t(a, b):
    return lax.dot_general(a, b, (((0,), (0,)), ((), ())), preferred_element_type=F32)


def iota(shape, dim):
    return lax.broadcasted_iota(jnp.int32, shape, dim)


def group_dz(g):
    dz = jnp.full_like(g, ORDER[0])
    for i in range(1, NG):
        dz = jnp.where(g == i, ORDER[i], dz)
    return dz


def kernel(
    x1_h, g1_h, pin_h, pmix_h, psc_h, pout_h, x2_h, g2_h, ids_h, lg_h, wg_h, wu_h, wd_h,
    out1, out2,
    ids, g2, g1, pmix, psc, lg, x1, pin, x2, wg, wu, wd, wg2, wu2,
    n1, pl_in, ext, halo, tail, plx, wo, xq,
    s, s1, s2, s3, r, lhs, hid, tm, rr, rv, fin, ret, fm, acc,
    sem_in, ws_s, ws_r, a_s, a_r, a2_s, n_s, n_r, g_s, g_r, y_s, y_r, v_s, v_r, d_s, d_r,
    b_s, b_r, h_s, h_r, wo_s, wo_r, wy_s, wy_r, wp_s, wp_r, p_s, p_r, p2_s, p2_r,
):
    ep, t = lax.axis_index("ep"), lax.axis_index("tp")
    c = lax.rem(ep, 2)
    chip = ep // 2
    y, z = lax.rem(chip, YN), chip // YN

    def at(dz, dy, dc=0):
        z2, y2, c2 = lax.rem(z + dz + ZN, ZN), lax.rem(y + dy + YN, YN), lax.rem(c + dc, 2)
        return ((z2 * YN + y2) * 2 + c2, t)

    def along(dx):
        return (ep, lax.rem(t + dx, XN))

    def quarter(dx):
        return lax.rem(t + dx + XN, XN)

    partner = at(0, 0, 1)
    following = (lax.rem(ep + 1, EP), t)
    previous = (lax.rem(ep + EP - 1, EP), t)

    def remote(src, dst, ss, rs, device):
        return pltpu.make_async_remote_copy(
            src_ref=src, dst_ref=dst, send_sem=ss, recv_sem=rs, device_id=device, device_id_type=MESH
        )

    def blocks_of(g, first=0, count=YN):
        return pl.ds(g * YN + first, count)

    loads = [
        pltpu.make_async_copy(a, b, sem_in.at[i])
        for i, (a, b) in enumerate(
            [(x2_h, x2), (x1_h, x1), (pin_h, pin), (wg_h.at[0], wg), (wu_h.at[0], wu), (wd_h.at[0], wd.at[pl.ds(0, 512)])]
        )
    ]
    small = [
        pltpu.make_async_copy(a, b, sem_in.at[7 + i])
        for i, (a, b) in enumerate([(ids_h, ids), (g2_h, g2), (g1_h, g1), (pmix_h, pmix), (psc_h, psc), (lg_h, lg)])
    ]
    for copy in small + loads:
        copy.start()

    bar = pltpu.get_barrier_semaphore()

    def greet(b, carry):
        pl.semaphore_signal(bar, inc=1, device_id=at(group_dz(b // YN), lax.rem(b, YN)), device_id_type=MESH)
        return carry

    lax.fori_loop(0, SELF, greet, 0)
    lax.fori_loop(SELF + 1, NB, greet, 0)
    for dx in (1, 2, 3):
        pl.semaphore_signal(bar, inc=1, device_id=along(dx), device_id_type=MESH)
    pl.semaphore_signal(bar, inc=1, device_id=partner, device_id_type=MESH)
    pl.semaphore_signal(bar, inc=1, device_id=previous, device_id_type=MESH)

    for copy in small:
        copy.wait()
    expert = iota((NB, 256), 0)
    one0 = (ids[0:1, :] == expert).astype(F32)
    one1 = (ids[1:2, :] == expert).astype(F32)
    earlier = (iota((256, 256), 0) < iota((256, 256), 1)).astype(BF16)
    place = dot((one0 + one1).astype(BF16), earlier) + 1.0

    def slot_maps(marks):
        held = (place * marks).astype(BF16)

        def spread(width, per):
            e, col = iota((NB, width), 0), iota((NB, width), 1) // per
            dz = group_dz(col // YN)
            hit = ((e // YN - z - dz + 2 * ZN) & (ZN - 1)) + ((lax.rem(e, YN) - y - lax.rem(col, YN) + 2 * YN) & (YN - 1))
            return dot_t(held, (hit == 0).astype(BF16))

        return spread(NB * 16, 16), spread(NB * 8, 8)

    slot_main = (lax.rem(iota((256, NB * 16), 1), 16) + 1).astype(F32)
    over_col = iota((256, NB * 8), 1)
    slot_over = (lax.rem(over_col // 4, 2) + 17).astype(F32)
    over_k = lax.rem(over_col, 4)

    loads[0].wait()

    def norm2(i, carry):
        rows = pl.ds(pl.multiple_of(i * 64, 64), 64)
        v = x2[rows, :].astype(F32)
        inv = lax.rsqrt(jnp.mean(v * v, axis=-1, keepdims=True) + EPS)
        for dx in range(4):
            cols = pl.ds(pl.multiple_of(quarter(-dx) * 512, 512), 512)
            xq[dx, rows, :] = (x2[rows, cols].astype(F32) * inv * g2[cols].astype(F32)).astype(BF16)
        return carry

    lax.fori_loop(0, 4, norm2, 0)
    in_main, in_over = slot_maps(one0 + one1)
    pick_main = (in_main == slot_main).astype(BF16)
    picks_over = [jnp.logical_and(in_over == slot_over, over_k == k).astype(BF16) for k in range(4)]

    def fill(buf, dx, skip):
        xv = xq[dx]
        count = NB - skip
        rows_main = dot_t(pick_main[:, skip * 16 :], xv)
        rows_over = jnp.zeros((count * 8, 128), F32)
        for k in range(4):
            lanes = slice(128 * k, 128 * k + 128)
            buf[:, 16 * k : 16 * k + 16, :] = rows_main[:, lanes].reshape(count, 16, 128).astype(BF16)
            rows_over = rows_over + dot_t(picks_over[k][:, skip * 8 :], xv[:, lanes])
        buf[:, 64:72, :] = rows_over.reshape(count, 8, 128).astype(BF16)
        r[dx, SELF] = buf[SELF - skip]

    fill(s, 0, 0)

    loads[1].wait()
    loads[2].wait()

    def normed1(rows):
        v = x1[rows, :].astype(F32)
        inv = lax.rsqrt(jnp.mean(v * v, axis=-1, keepdims=True) + EPS)
        return (v * inv * g1[...].astype(F32)).astype(BF16)

    tail[...] = dot(normed1(pl.ds(496, 16)), pin[...]).astype(BF16)
    halo_copy = remote(tail, halo, h_s, h_r, following)

    pl.semaphore_wait(bar, NB - 1 + 3 + 2)

    halo_copy.start()

    def toward(b):
        return at(group_dz(b // YN), lax.rem(b, YN))

    def send_blocks(buf, dx, skip, g, ss, arrival):
        def body(dy, carry):
            b = g * YN + dy
            remote(buf.at[b - skip], r.at[dx, b], ss, arrival, at(ORDER[g], dy)).start()
            return carry

        lax.fori_loop(1 if ORDER[g] == 0 else 0, YN, body, 0)

    half_rows = pl.ds(pl.multiple_of(c * 128, 128), 128)
    piece = pl.ds(pl.multiple_of(c * 128 + y * 32, 32), 32)
    outward = []
    for dx in (1, 2, 3):
        cols = pl.ds(pl.multiple_of(quarter(dx) * 512, 512), 512)
        outward.append(remote(pout_h.at[piece, cols], wo.at[dx, piece], wo_s, wo_r, along(dx)))
    for copy in outward:
        copy.start()
    along_y = [
        remote(wo.at[pl.ds(1, 3), piece], wo.at[pl.ds(1, 3), piece], wy_s, wy_r, at(0, dy)) for dy in (1, 2, 3)
    ]
    shared = remote(wo.at[pl.ds(1, 3), half_rows], wo.at[pl.ds(1, 3), half_rows], wp_s, wp_r, partner)
    for g in range(NR):
        send_blocks(s, 0, 0, g, a_s, a_r.at[g])
    send_blocks(s, 0, 0, NR, a_s, n_r.at[0])

    swaps = [
        remote(a, b, ws_s.at[i], ws_r.at[i], partner)
        for i, (a, b) in enumerate([(wg_h.at[0], wg2), (wu_h.at[0], wu2), (wd_h.at[0], wd.at[pl.ds(512, 512)])])
    ]
    for copy in swaps:
        copy.start()

    own_out = pltpu.make_async_copy(
        pout_h.at[:, pl.ds(pl.multiple_of(t * 512, 512), 512)], wo.at[0], sem_in.at[6]
    )
    own_out.start()

    def landed(ref, sem):
        remote(ref, ref, a_s, sem, partner).wait_recv()

    def left(ref, sem):
        remote(ref, ref, sem, a_r.at[0], partner).wait_send()

    def gather(g, dx):
        rows = blocks_of(g)
        arrival = g_r.at[2 * g + dx // 2 if g < NR - 1 else g // 4 + 2 * NR - 2]
        return remote(r.at[0, rows], r.at[dx, rows], g_s, arrival, along(dx))

    def relay(g, dx):
        rows = blocks_of(g, dx - 1, 2)
        return remote(r.at[dx, rows], r.at[2, rows], y_s, y_r, along(dx))

    def arrived(g):
        landed(s.at[pl.ds(0, YN)], a_r.at[g])

    def pass_on(g):
        arrived(g)
        for dx in ((1, 3), (1, 3), (1, 3, 2), (), (3,), (1,))[g]:
            gather(g, dx).start()

    def relay_on(g):
        for dx in (1, 3):
            gather(g, dx).wait_recv()
            relay(g, dx).start()

    def norm1(i, carry):
        rows = pl.ds(pl.multiple_of(i * 64, 64), 64)
        n1[rows, :] = normed1(rows)
        return carry

    lax.fori_loop(0, 8, norm1, 0)
    def inward(i, carry):
        rows = pl.ds(pl.multiple_of(i * 256, 256), 256)
        pl_in[rows, :] = dot(n1[rows, :], pin[...]).astype(BF16)
        return carry

    lax.fori_loop(0, 2, inward, 0)

    halo_copy.wait_recv()
    ext[0:16, :] = jnp.where(ep == 0, 0.0, halo[...].astype(F32))
    ext[16:528, :] = pl_in[...].astype(F32)
    window = jnp.left_shift(jnp.int32(2), t)
    reach = ext[...]
    total = jnp.zeros((528, 256), F32)
    for i in range(4):
        reach = reach + pltpu.roll(reach, 1 << i, 0)
        total = jnp.where(t == i, reach, total)
    count = jnp.minimum(ep * 512 + iota((512, 1), 0) + 1, window).astype(F32)
    mixed = (total[16:528, :] / count - ext[16:528, :]).astype(BF16)
    plx[0] = (dot(mixed, pmix[0]) * psc[...].astype(F32)).astype(BF16)
    def pooled(dx):
        return remote(plx.at[0], plx.at[dx], p_s, p_r.at[dx // 2], along(dx))

    def pooled_on(dx):
        rows = pl.ds(128 * (dx - 1), 256)
        return remote(plx.at[dx, rows], plx.at[2, rows], p2_s, p2_r, along(dx))

    for dx in (1, 3):
        pooled(dx).start()

    for dx in (1, 2, 3):
        fill((s1, s2, s3)[dx - 1], dx, NR * YN)
    for g in (3, 4, 5, 6, 7):
        whole = ORDER[g] in (0, 1, 7)
        for buf, dx, ss in ((s, 0, a_s), (s2, 2, a2_s), (s1, 1, n_s), (s3, 3, n_s)):
            if dx == 0 and g > NR:
                send_blocks(s, 0, 0, g, a_s, n_r.at[2] if whole else a_r.at[g])
            elif dx == 2 or (dx and whole) or (g, dx) in ((4, 1), (5, 3)):
                send_blocks(buf, dx, NR * YN, g, ss, n_r.at[0 if g == NR else 2 if whole else 1])
    pass_on(0)
    pass_on(1)
    relay_on(0)
    relay_on(1)
    pass_on(2)
    pass_on(4)
    pass_on(5)
    landed(wo.at[pl.ds(1, 3), piece], wo_r)
    for copy in along_y:
        copy.start()

    def expand(k):
        m, n = iota((PAIR * 2, PAIR * 8), 0), iota((PAIR * 2, PAIR * 8), 1)
        return (n == (m // 2) * 8 + lax.rem(m, 2) * 4 + k).astype(BF16)

    def rows_in(i):
        blocks = pl.ds(i * PAIR, PAIR)
        for dx in range(4):
            q = quarter(-dx)
            over = r[dx, blocks, 64:72, :].astype(F32).reshape(PAIR * 8, 128).astype(BF16)
            for k in range(4):
                cols = pl.ds(pl.multiple_of(q * 512 + 128 * k, 128), 128)
                lhs[0 : PAIR * 16, cols] = r[dx, blocks, 16 * k : 16 * k + 16, :].reshape(PAIR * 16, 128)
                lhs[PAIR * 16 : PAIR * 18, cols] = dot(expand(k), over).astype(BF16)

    def units(n, carry):
        cols = pl.ds(n * 256, 256) if isinstance(n, int) else pl.ds(pl.multiple_of(n * 256, 256), 256)
        for j, (a, b) in enumerate([(wg, wu), (wg2, wu2)]):
            gate, up = dot(lhs[...], a[:, cols]), dot(lhs[...], b[:, cols])
            hid[:, pl.ds(512 * j + n * 256, 256) if isinstance(n, int) else pl.ds(pl.multiple_of(512 * j + n * 256, 256), 256)] = (gate / (1.0 + jnp.exp(-gate)) * up).astype(BF16)
        return carry

    def down(i, dx):
        blocks = pl.ds(i * PAIR, PAIR)
        cols = pl.ds(pl.multiple_of(quarter(dx) * 512, 512), 512)
        term = dot(hid[...], wd[:, cols])
        n, m = iota((PAIR * 8, PAIR * 2), 0), iota((PAIR * 8, PAIR * 2), 1)
        spread = dot((n // 4 == m).astype(BF16), term[PAIR * 16 :].astype(BF16))
        lane_group = lax.rem(iota((PAIR * 8, 128), 0), 4)
        over = spread[:, 0:128]
        for k in range(4):
            part = term[0 : PAIR * 16, 128 * k : 128 * k + 128]
            tm[dx, blocks, 16 * k : 16 * k + 16, :] = part.reshape(PAIR, 16, 128).astype(BF16)
            if k:
                over = jnp.where(lane_group == k, spread[:, 128 * k : 128 * k + 128], over)
        tm[dx, blocks, 64:72, :] = over.reshape(PAIR, 8, 128).astype(BF16)

    def by_way(j, dx):
        rows = blocks_of(2 * j + dx // 2)
        return remote(tm.at[2, rows], rv.at[rows], v_s, v_r.at[dx // 2, j], along(dx))

    def direct(j, dx):
        g = 2 * j + 1 - dx // 2
        rows = blocks_of(g)
        return remote(tm.at[dx, rows], rr.at[dx // 2, rows], d_s, d_r.at[g], along(dx))

    def joined(j, dx):
        g = 2 * j + dx // 2
        rows = blocks_of(g)
        return remote(tm.at[dx, rows], rr.at[dx // 2, rows], d_s, d_r.at[g], along(dx))

    def each(first, last, action):
        def body(g, carry):
            action(g)
            return carry

        lax.fori_loop(first, last, body, 0)

    def start_by_way(j):
        for dx in (1, 3):
            by_way(j, dx).start()

    def join(j):
        for dx in (1, 3):
            by_way(j, dx).wait_recv()
            rows = blocks_of(2 * j + dx // 2)
            tm[dx, rows] = (tm[dx, rows].astype(F32) + rv[rows].astype(F32)).astype(BF16)
            joined(j, dx).start()

    def back(b):
        return remote(fin.at[b], ret.at[b], b_s, b_r.at[b // (4 * YN)], at(ZN - group_dz(b // YN), YN - lax.rem(b, YN)))

    def summed(g):
        rows = blocks_of(g)
        landed(s.at[pl.ds(0, 2 * YN)], d_r.at[g])
        v = tm[0, rows].astype(F32) + rr[0, rows].astype(F32) + rr[1, rows].astype(F32)
        fin[rows] = v.astype(BF16)

    def give_back(g):
        summed(g)
        for dy in range(YN):
            back(g * YN + dy).start()

    def up_part(j):
        with jax.named_scope(f"rows{j}"):
            rows_in(j)
        with jax.named_scope(f"units{j}"):
            lax.fori_loop(0, 2, units, 0)

    def down_part(j):
        with jax.named_scope(f"down{j}"):
            down(j, 2)
            start_by_way(j)
            for dx in (1, 3, 0):
                down(j, dx)
            for dx in (1, 3):
                direct(j, dx).start()

    landed(s.at[pl.ds(0, PAIR)], y_r)
    for copy in loads[3:]:
        copy.wait()
    for copy in swaps:
        copy.wait_recv()
    up_part(0)
    down_part(0)
    landed(s.at[pl.ds(0, NR * YN)], g_r.at[2 * NR - 2])
    landed(s.at[pl.ds(0, NR * YN)], n_r.at[0])
    up_part(1)
    down_part(1)
    join(0)
    landed(s.at[pl.ds(0, PAIR)], g_r.at[2 * NR - 1])
    landed(s.at[pl.ds(0, 4 * YN)], n_r.at[1])
    up_part(2)
    down_part(2)
    join(1)
    landed(wo.at[pl.ds(1, 3), pl.ds(0, 96)], wy_r)
    shared.start()
    landed(s, n_r.at[2])
    up_part(3)
    each(0, 2, give_back)
    down_part(3)
    join(2)
    give_back(2)
    summed(NR)
    ret[SELF] = fin[SELF]
    for dy in range(1, YN):
        back(SELF + dy).start()
    join(3)
    for dx in (1, 3):
        pooled(dx).wait_recv()
        pooled_on(dx).start()
    each(4, NG, give_back)

    row0 = iota((8, 256), 0) == 0
    gap = lg[1:2, :] - lg[0:1, :]
    shares = jnp.where(row0, 1.0 / (1.0 + jnp.exp(gap)), 1.0 / (1.0 + jnp.exp(-gap))).T
    maps = [(slot_maps(one0), shares[:, 0:1]), (slot_maps(one1), shares[:, 1:2])]
    own_out.wait()
    shared.wait_recv()
    landed(plx.at[0], p2_r)
    for n in range(2):
        rows = slice(256 * n, 256 * n + 256)
        mixed_out = dot(plx[0, rows, :], wo[0])
        for dx in (1, 2, 3):
            mixed_out = mixed_out + dot(plx[dx, rows, :], wo[dx])
        out1[rows, :] = mixed_out.astype(BF16)

    def pick_up(i):
        blocks = pl.ds(16 * i, 16)
        for k in range(4):
            fm[:, 128 * k : 128 * k + 128] = ret[blocks, 16 * k : 16 * k + 16, :].reshape(256, 128)
        fo = ret[blocks, 64:72, :].astype(F32).reshape(128, 128).astype(BF16)
        values = []
        for (main, over), share in maps:
            lanes = slice(256 * i, 256 * i + 256)
            base = dot((main[:, lanes] == slot_main[:, lanes]).astype(BF16), fm[...])
            lanes = slice(128 * i, 128 * i + 128)
            hits = over[:, lanes] == slot_over[:, lanes]
            marks = [jnp.logical_and(hits, over_k[:, lanes] == k).astype(BF16) for k in range(4)]
            extra = [dot(mark, fo) for mark in marks]
            values.append((base, extra, share))
        return [
            sum(share * (base[:, 128 * k : 128 * k + 128] + extra[k]) for base, extra, share in values) for k in range(4)
        ]

    landed(s.at[pl.ds(0, 15)], b_r.at[0])
    for k, v in enumerate(pick_up(0)):
        acc[:, 128 * k : 128 * k + 128] = v
    landed(s.at[pl.ds(0, 16)], b_r.at[1])
    for k, v in enumerate(pick_up(1)):
        lanes = slice(128 * k, 128 * k + 128)
        out2[:, lanes] = (acc[:, lanes] + v).astype(BF16)

    left(s.at[pl.ds(0, NB - 1)], a_s)
    left(s.at[pl.ds(0, NB - NR * YN - 1)], a2_s)
    left(s.at[pl.ds(0, 30)], n_s)
    left(r.at[pl.ds(0, 2), pl.ds(0, 18)], g_s)
    left(s.at[pl.ds(0, (NR - 1) * YN)], y_s)
    left(s, v_s)
    left(r.at[pl.ds(0, 2)], d_s)
    left(s.at[pl.ds(0, NB - 1)], b_s)
    left(plx.at[pl.ds(0, 2)], p_s)
    left(plx.at[0], p2_s)
    left(wo.at[pl.ds(1, 3), piece], wo_s)
    left(wo.at[pl.ds(1, 3), pl.ds(0, 96)], wy_s)
    for copy in swaps + [shared, halo_copy]:
        copy.wait_send()


def local(
    first_input, first_gain, pool_inward, pool_mixing, pool_scale, pool_outward,
    second_input, second_gain, route_ids, route_logits, expert_gate, expert_up, expert_down,
):
    vmem = pl.BlockSpec(memory_space=pltpu.VMEM)
    far = pl.BlockSpec(memory_space=pl.ANY)
    dma = pltpu.SemaphoreType.DMA
    m = PAIR * 18
    return pl.pallas_call(
        kernel,
        name="mixer_experts",
        out_shape=(pltpu.VMEM((512, 512), BF16), pltpu.VMEM((256, 512), BF16)),
        in_specs=[far] * 13,
        out_specs=(vmem, vmem),
        scratch_shapes=[
            pltpu.VMEM((2, 256), jnp.int32),
            pltpu.VMEM((2048,), BF16),
            pltpu.VMEM((2048,), BF16),
            pltpu.VMEM((1, 256, 256), BF16),
            pltpu.VMEM((256,), BF16),
            pltpu.VMEM((2, 256), F32),
            pltpu.VMEM((512, 2048), BF16),
            pltpu.VMEM((2048, 256), BF16),
            pltpu.VMEM((256, 2048), BF16),
            pltpu.VMEM((2048, 512), BF16),
            pltpu.VMEM((2048, 512), BF16),
            pltpu.VMEM((1024, 2048), BF16),
            pltpu.VMEM((2048, 512), BF16),
            pltpu.VMEM((2048, 512), BF16),
            pltpu.VMEM((512, 2048), BF16),
            pltpu.VMEM((512, 256), BF16),
            pltpu.VMEM((528, 256), F32),
            pltpu.VMEM((16, 256), BF16),
            pltpu.VMEM((16, 256), BF16),
            pltpu.VMEM((4, 512, 256), BF16),
            pltpu.VMEM((4, 256, 512), BF16),
            pltpu.VMEM((4, 256, 512), BF16),
            pltpu.VMEM((NB, 72, 128), BF16),
            pltpu.VMEM((NB - NR * YN, 72, 128), BF16),
            pltpu.VMEM((NB - NR * YN, 72, 128), BF16),
            pltpu.VMEM((NB - NR * YN, 72, 128), BF16),
            pltpu.VMEM((4, NB, 72, 128), BF16),
            pltpu.VMEM((m, 2048), BF16),
            pltpu.VMEM((m, 1024), BF16),
            pltpu.VMEM((4, NB, 72, 128), BF16),
            pltpu.VMEM((2, NB, 72, 128), BF16),
            pltpu.VMEM((NB, 72, 128), BF16),
            pltpu.VMEM((NB, 72, 128), BF16),
            pltpu.VMEM((NB, 72, 128), BF16),
            pltpu.VMEM((256, 512), BF16),
            pltpu.VMEM((256, 512), F32),
            dma((13,)),
            dma((3,)), dma((3,)),
            dma, dma((6,)),
            dma, dma, dma((3,)),
            dma, dma((2 * NR,)),
            dma, dma,
            dma, dma((2, 4)),
            dma, dma((NG,)),
            dma, dma((2,)),
            dma, dma,
            dma, dma,
            dma, dma,
            dma, dma,
            dma, dma((2,)),
            dma, dma,
        ],
        compiler_params=pltpu.CompilerParams(
            collective_id=0, has_side_effects=True, vmem_limit_bytes=64000 * 1024
        ),
    )(
        first_input, first_gain, pool_inward, pool_mixing, pool_scale, pool_outward,
        second_input, second_gain, route_ids.T, route_logits.T, expert_gate, expert_up, expert_down,
    )


def solution(mesh):
    placed = (
        P("ep", None), P(), P(None, "tp"), P("tp", None, None), P("tp"), P("tp", None),
        P("ep", None), P(), P("ep", None), P("ep", None),
        P("ep", None, "tp"), P("ep", None, "tp"), P("ep", "tp", None),
    )
    return jax.shard_map(
        local, mesh=mesh, in_specs=placed, out_specs=(P("ep", "tp"), P("ep", "tp")), check_vma=False
    )
```

```python
import jax
import jax.numpy as jnp
from jax import lax
from jax.experimental import pallas as pl
from jax.experimental.pallas import tpu as pltpu
from jax.sharding import PartitionSpec as P

MESH = pl.DeviceIdType.MESH
F32, BF16 = jnp.float32, jnp.bfloat16
EPS = 1e-06
ZN, YN, XN = 8, 4, 4
NB = ZN * YN
NG = ZN
EP = NB * 2
PAIR = 2 * YN
ORDER = (3, 5, 4, 0, 2, 6, 1, 7)
NR = 3
SELF = 3 * YN


def dot(a, b):
    return jnp.dot(a, b, preferred_element_type=F32)


def dot_t(a, b):
    return lax.dot_general(a, b, (((0,), (0,)), ((), ())), preferred_element_type=F32)


def iota(shape, dim):
    return lax.broadcasted_iota(jnp.int32, shape, dim)


def group_dz(g):
    dz = jnp.full_like(g, ORDER[0])
    for i in range(1, NG):
        dz = jnp.where(g == i, ORDER[i], dz)
    return dz


def kernel(
    x1_h, g1_h, pin_h, pmix_h, psc_h, pout_h, x2_h, g2_h, ids_h, lg_h, wg_h, wu_h, wd_h,
    out1, out2,
    ids, g2, g1, pmix, psc, lg, x1, pin, x2, wg, wu, wd, wg2, wu2,
    n1, pl_in, ext, halo, tail, plx, wo, xq,
    s, s1, s2, s3, r, lhs, hid, tm, rr, rv, fin, ret, fm, acc,
    sem_in, ws_s, ws_r, a_s, a_r, a2_s, n_s, n_r, g_s, g_r, y_s, y_r, v_s, v_r, d_s, d_r,
    b_s, b_r, h_s, h_r, wo_s, wo_r, wy_s, wy_r, wp_s, wp_r, p_s, p_r, p2_s, p2_r,
):
    ep, t = lax.axis_index("ep"), lax.axis_index("tp")
    c = lax.rem(ep, 2)
    chip = ep // 2
    y, z = lax.rem(chip, YN), chip // YN

    def at(dz, dy, dc=0):
        z2, y2, c2 = (z + dz + ZN) & (ZN - 1), (y + dy + YN) & (YN - 1), (c + dc) & 1
        return ((z2 * YN + y2) * 2 + c2, t)

    def along(dx):
        return (ep, (t + dx) & (XN - 1))

    def quarter(dx):
        return (t + dx + XN) & (XN - 1)

    partner = at(0, 0, 1)
    following = (lax.rem(ep + 1, EP), t)
    previous = (lax.rem(ep + EP - 1, EP), t)

    def remote(src, dst, ss, rs, device):
        return pltpu.make_async_remote_copy(
            src_ref=src, dst_ref=dst, send_sem=ss, recv_sem=rs, device_id=device, device_id_type=MESH
        )

    def blocks_of(g, first=0, count=YN):
        return pl.ds(g * YN + first, count)

    loads = [
        pltpu.make_async_copy(a, b, sem_in.at[i])
        for i, (a, b) in enumerate(
            [(x2_h, x2), (x1_h, x1), (pin_h, pin), (wg_h.at[0], wg), (wu_h.at[0], wu), (wd_h.at[0], wd.at[pl.ds(0, 512)])]
        )
    ]
    small = [
        pltpu.make_async_copy(a, b, sem_in.at[7 + i])
        for i, (a, b) in enumerate([(ids_h, ids), (g2_h, g2), (g1_h, g1), (pmix_h, pmix), (psc_h, psc), (lg_h, lg)])
    ]
    for copy in small + loads:
        copy.start()

    bar = pltpu.get_barrier_semaphore()

    for b in range(NB):
        if b != SELF:
            pl.semaphore_signal(bar, inc=1, device_id=at(ORDER[b // YN], b % YN), device_id_type=MESH)
    for dx in (1, 2, 3):
        pl.semaphore_signal(bar, inc=1, device_id=along(dx), device_id_type=MESH)
    pl.semaphore_signal(bar, inc=1, device_id=partner, device_id_type=MESH)
    pl.semaphore_signal(bar, inc=1, device_id=previous, device_id_type=MESH)

    for copy in small:
        copy.wait()
    expert = iota((NB, 256), 0)
    one0 = (ids[0:1, :] == expert).astype(F32)
    one1 = (ids[1:2, :] == expert).astype(F32)
    earlier = (iota((256, 256), 0) < iota((256, 256), 1)).astype(BF16)
    place = dot((one0 + one1).astype(BF16), earlier) + 1.0

    def slot_maps(marks):
        held = (place * marks).astype(BF16)

        def spread(width, per):
            e, col = iota((NB, width), 0), iota((NB, width), 1) // per
            dz = group_dz(col // YN)
            hit = ((e // YN - z - dz + 2 * ZN) & (ZN - 1)) + ((lax.rem(e, YN) - y - lax.rem(col, YN) + 2 * YN) & (YN - 1))
            return dot_t(held, (hit == 0).astype(BF16))

        return spread(NB * 16, 16), spread(NB * 8, 8)

    slot_main = (lax.rem(iota((256, NB * 16), 1), 16) + 1).astype(F32)
    over_col = iota((256, NB * 8), 1)
    slot_over = (lax.rem(over_col // 4, 2) + 17).astype(F32)
    over_k = lax.rem(over_col, 4)

    loads[0].wait()

    def norm2(i, carry):
        rows = pl.ds(pl.multiple_of(i * 64, 64), 64)
        v = x2[rows, :].astype(F32)
        inv = lax.rsqrt(jnp.mean(v * v, axis=-1, keepdims=True) + EPS)
        for dx in range(4):
            cols = pl.ds(pl.multiple_of(quarter(-dx) * 512, 512), 512)
            xq[dx, rows, :] = (x2[rows, cols].astype(F32) * inv * g2[cols].astype(F32)).astype(BF16)
        return carry

    lax.fori_loop(0, 4, norm2, 0)
    in_main, in_over = slot_maps(one0 + one1)
    pick_main = (in_main == slot_main).astype(BF16)
    picks_over = [jnp.logical_and(in_over == slot_over, over_k == k).astype(BF16) for k in range(4)]

    def fill(buf, dx, skip):
        xv = xq[dx]
        count = NB - skip
        rows_main = dot_t(pick_main[:, skip * 16 :], xv)
        rows_over = jnp.zeros((count * 8, 128), F32)
        for k in range(4):
            lanes = slice(128 * k, 128 * k + 128)
            buf[:, 16 * k : 16 * k + 16, :] = rows_main[:, lanes].reshape(count, 16, 128).astype(BF16)
            rows_over = rows_over + dot_t(picks_over[k][:, skip * 8 :], xv[:, lanes])
        buf[:, 64:72, :] = rows_over.reshape(count, 8, 128).astype(BF16)
        r[dx, SELF] = buf[SELF - skip]

    fill(s, 0, 0)

    loads[1].wait()
    loads[2].wait()

    def normed1(rows):
        v = x1[rows, :].astype(F32)
        inv = lax.rsqrt(jnp.mean(v * v, axis=-1, keepdims=True) + EPS)
        return (v * inv * g1[...].astype(F32)).astype(BF16)

    tail[...] = dot(normed1(pl.ds(496, 16)), pin[...]).astype(BF16)
    halo_copy = remote(tail, halo, h_s, h_r, following)

    pl.semaphore_wait(bar, NB - 1 + 3 + 2)

    halo_copy.start()

    def toward(b):
        return at(group_dz(b // YN), lax.rem(b, YN))

    def send_blocks(buf, dx, skip, g, ss, arrival):
        def body(dy, carry):
            b = g * YN + dy
            remote(buf.at[b - skip], r.at[dx, b], ss, arrival, at(ORDER[g], dy)).start()
            return carry

        lax.fori_loop(1 if ORDER[g] == 0 else 0, YN, body, 0)

    half_rows = pl.ds(pl.multiple_of(c * 128, 128), 128)
    piece = pl.ds(pl.multiple_of(c * 128 + y * 32, 32), 32)
    outward = []
    for dx in (1, 2, 3):
        cols = pl.ds(pl.multiple_of(quarter(dx) * 512, 512), 512)
        outward.append(remote(pout_h.at[piece, cols], wo.at[dx, piece], wo_s, wo_r, along(dx)))
    for copy in outward:
        copy.start()
    along_y = [
        remote(wo.at[pl.ds(1, 3), piece], wo.at[pl.ds(1, 3), piece], wy_s, wy_r, at(0, dy)) for dy in (1, 2, 3)
    ]
    shared = remote(wo.at[pl.ds(1, 3), half_rows], wo.at[pl.ds(1, 3), half_rows], wp_s, wp_r, partner)
    for g in range(NR):
        send_blocks(s, 0, 0, g, a_s, a_r.at[g])
    send_blocks(s, 0, 0, NR, a_s, n_r.at[0])

    swaps = [
        remote(a, b, ws_s.at[i], ws_r.at[i], partner)
        for i, (a, b) in enumerate([(wg_h.at[0], wg2), (wu_h.at[0], wu2), (wd_h.at[0], wd.at[pl.ds(512, 512)])])
    ]
    for copy in swaps:
        copy.start()

    own_out = pltpu.make_async_copy(
        pout_h.at[:, pl.ds(pl.multiple_of(t * 512, 512), 512)], wo.at[0], sem_in.at[6]
    )
    own_out.start()

    def landed(ref, sem):
        remote(ref, ref, a_s, sem, partner).wait_recv()

    def left(ref, sem):
        remote(ref, ref, sem, a_r.at[0], partner).wait_send()

    def gather(g, dx):
        rows = blocks_of(g)
        arrival = g_r.at[2 * g + dx // 2 if g < NR - 1 else g // 4 + 2 * NR - 2]
        return remote(r.at[0, rows], r.at[dx, rows], g_s, arrival, along(dx))

    def relay(g, dx):
        rows = blocks_of(g, dx - 1, 2)
        return remote(r.at[dx, rows], r.at[2, rows], y_s, y_r, along(dx))

    def arrived(g):
        landed(s.at[pl.ds(0, YN)], a_r.at[g])

    def pass_on(g):
        arrived(g)
        for dx in ((1, 3), (1, 3), (1, 3, 2), (), (3,), (1,))[g]:
            gather(g, dx).start()

    def relay_on(g):
        for dx in (1, 3):
            gather(g, dx).wait_recv()
            relay(g, dx).start()

    def norm1(i, carry):
        rows = pl.ds(pl.multiple_of(i * 64, 64), 64)
        n1[rows, :] = normed1(rows)
        return carry

    lax.fori_loop(0, 8, norm1, 0)
    def inward(i, carry):
        rows = pl.ds(pl.multiple_of(i * 256, 256), 256)
        pl_in[rows, :] = dot(n1[rows, :], pin[...]).astype(BF16)
        return carry

    lax.fori_loop(0, 2, inward, 0)

    halo_copy.wait_recv()
    ext[0:16, :] = jnp.where(ep == 0, 0.0, halo[...].astype(F32))
    ext[16:528, :] = pl_in[...].astype(F32)
    window = jnp.left_shift(jnp.int32(2), t)
    reach = ext[...]
    total = jnp.zeros((528, 256), F32)
    for i in range(4):
        reach = reach + pltpu.roll(reach, 1 << i, 0)
        total = jnp.where(t == i, reach, total)
    count = jnp.minimum(ep * 512 + iota((512, 1), 0) + 1, window).astype(F32)
    mixed = (total[16:528, :] / count - ext[16:528, :]).astype(BF16)
    plx[0] = (dot(mixed, pmix[0]) * psc[...].astype(F32)).astype(BF16)
    def pooled(dx):
        return remote(plx.at[0], plx.at[dx], p_s, p_r.at[dx // 2], along(dx))

    def pooled_on(dx):
        rows = pl.ds(128 * (dx - 1), 256)
        return remote(plx.at[dx, rows], plx.at[2, rows], p2_s, p2_r, along(dx))

    for dx in (1, 3):
        pooled(dx).start()

    for dx in (1, 2, 3):
        fill((s1, s2, s3)[dx - 1], dx, NR * YN)
    for g in (3, 4, 5, 6, 7):
        whole = ORDER[g] in (0, 1, 7)
        for buf, dx, ss in ((s, 0, a_s), (s2, 2, a2_s), (s1, 1, n_s), (s3, 3, n_s)):
            if dx == 0 and g > NR:
                send_blocks(s, 0, 0, g, a_s, n_r.at[2] if whole else a_r.at[g])
            elif dx == 2 or (dx and whole) or (g, dx) in ((4, 1), (5, 3)):
                send_blocks(buf, dx, NR * YN, g, ss, n_r.at[0 if g == NR else 2 if whole else 1])
    pass_on(0)
    pass_on(1)
    relay_on(0)
    relay_on(1)
    pass_on(2)
    pass_on(4)
    pass_on(5)
    landed(wo.at[pl.ds(1, 3), piece], wo_r)
    for copy in along_y:
        copy.start()

    def expand(k):
        m, n = iota((PAIR * 2, PAIR * 8), 0), iota((PAIR * 2, PAIR * 8), 1)
        return (n == (m // 2) * 8 + lax.rem(m, 2) * 4 + k).astype(BF16)

    def rows_in(i):
        blocks = pl.ds(i * PAIR, PAIR)
        for dx in range(4):
            q = quarter(-dx)
            over = r[dx, blocks, 64:72, :].astype(F32).reshape(PAIR * 8, 128).astype(BF16)
            for k in range(4):
                cols = pl.ds(pl.multiple_of(q * 512 + 128 * k, 128), 128)
                lhs[0 : PAIR * 16, cols] = r[dx, blocks, 16 * k : 16 * k + 16, :].reshape(PAIR * 16, 128)
                lhs[PAIR * 16 : PAIR * 18, cols] = dot(expand(k), over).astype(BF16)

    def units(n, carry):
        cols = pl.ds(n * 256, 256) if isinstance(n, int) else pl.ds(pl.multiple_of(n * 256, 256), 256)
        for j, (a, b) in enumerate([(wg, wu), (wg2, wu2)]):
            gate, up = dot(lhs[...], a[:, cols]), dot(lhs[...], b[:, cols])
            hid[:, pl.ds(512 * j + n * 256, 256) if isinstance(n, int) else pl.ds(pl.multiple_of(512 * j + n * 256, 256), 256)] = (gate / (1.0 + jnp.exp(-gate)) * up).astype(BF16)
        return carry

    def down(i, dx):
        blocks = pl.ds(i * PAIR, PAIR)
        cols = pl.ds(pl.multiple_of(quarter(dx) * 512, 512), 512)
        term = dot(hid[...], wd[:, cols])
        n, m = iota((PAIR * 8, PAIR * 2), 0), iota((PAIR * 8, PAIR * 2), 1)
        spread = dot((n // 4 == m).astype(BF16), term[PAIR * 16 :].astype(BF16))
        lane_group = lax.rem(iota((PAIR * 8, 128), 0), 4)
        over = spread[:, 0:128]
        for k in range(4):
            part = term[0 : PAIR * 16, 128 * k : 128 * k + 128]
            tm[dx, blocks, 16 * k : 16 * k + 16, :] = part.reshape(PAIR, 16, 128).astype(BF16)
            if k:
                over = jnp.where(lane_group == k, spread[:, 128 * k : 128 * k + 128], over)
        tm[dx, blocks, 64:72, :] = over.reshape(PAIR, 8, 128).astype(BF16)

    def by_way(j, dx):
        rows = blocks_of(2 * j + dx // 2)
        return remote(tm.at[2, rows], rv.at[rows], v_s, v_r.at[dx // 2, j], along(dx))

    def direct(j, dx):
        g = 2 * j + 1 - dx // 2
        rows = blocks_of(g)
        return remote(tm.at[dx, rows], rr.at[dx // 2, rows], d_s, d_r.at[g], along(dx))

    def joined(j, dx):
        g = 2 * j + dx // 2
        rows = blocks_of(g)
        return remote(tm.at[dx, rows], rr.at[dx // 2, rows], d_s, d_r.at[g], along(dx))

    def each(first, last, action):
        def body(g, carry):
            action(g)
            return carry

        lax.fori_loop(first, last, body, 0)

    def start_by_way(j):
        for dx in (1, 3):
            by_way(j, dx).start()

    def join(j):
        for dx in (1, 3):
            by_way(j, dx).wait_recv()
            rows = blocks_of(2 * j + dx // 2)
            tm[dx, rows] = (tm[dx, rows].astype(F32) + rv[rows].astype(F32)).astype(BF16)
            joined(j, dx).start()

    def back(b):
        return remote(fin.at[b], ret.at[b], b_s, b_r.at[b // (4 * YN)], at(ZN - group_dz(b // YN), YN - lax.rem(b, YN)))

    def summed(g):
        rows = blocks_of(g)
        landed(s.at[pl.ds(0, 2 * YN)], d_r.at[g])
        v = tm[0, rows].astype(F32) + rr[0, rows].astype(F32) + rr[1, rows].astype(F32)
        fin[rows] = v.astype(BF16)

    def give_back(g):
        summed(g)
        for dy in range(YN):
            back(g * YN + dy).start()

    def up_part(j):
        with jax.named_scope(f"rows{j}"):
            rows_in(j)
        with jax.named_scope(f"units{j}"):
            lax.fori_loop(0, 2, units, 0)

    def down_part(j):
        with jax.named_scope(f"down{j}"):
            down(j, 2)
            start_by_way(j)
            for dx in (1, 3, 0):
                down(j, dx)
            for dx in (1, 3):
                direct(j, dx).start()

    landed(s.at[pl.ds(0, PAIR)], y_r)
    for copy in loads[3:]:
        copy.wait()
    for copy in swaps:
        copy.wait_recv()
    up_part(0)
    down_part(0)
    landed(s.at[pl.ds(0, NR * YN)], g_r.at[2 * NR - 2])
    landed(s.at[pl.ds(0, NR * YN)], n_r.at[0])
    up_part(1)
    down_part(1)
    join(0)
    landed(s.at[pl.ds(0, PAIR)], g_r.at[2 * NR - 1])
    landed(s.at[pl.ds(0, 4 * YN)], n_r.at[1])
    up_part(2)
    down_part(2)
    join(1)
    landed(wo.at[pl.ds(1, 3), pl.ds(0, 96)], wy_r)
    shared.start()
    landed(s, n_r.at[2])
    up_part(3)
    each(0, 2, give_back)
    down_part(3)
    join(2)
    give_back(2)
    summed(NR)
    ret[SELF] = fin[SELF]
    for dy in range(1, YN):
        back(SELF + dy).start()
    join(3)
    for dx in (1, 3):
        pooled(dx).wait_recv()
        pooled_on(dx).start()
    each(4, NG, give_back)

    row0 = iota((8, 256), 0) == 0
    gap = lg[1:2, :] - lg[0:1, :]
    shares = jnp.where(row0, 1.0 / (1.0 + jnp.exp(gap)), 1.0 / (1.0 + jnp.exp(-gap))).T
    maps = [(slot_maps(one0), shares[:, 0:1]), (slot_maps(one1), shares[:, 1:2])]
    own_out.wait()
    shared.wait_recv()
    landed(plx.at[0], p2_r)
    for n in range(2):
        rows = slice(256 * n, 256 * n + 256)
        mixed_out = dot(plx[0, rows, :], wo[0])
        for dx in (1, 2, 3):
            mixed_out = mixed_out + dot(plx[dx, rows, :], wo[dx])
        out1[rows, :] = mixed_out.astype(BF16)

    def pick_up(i):
        blocks = pl.ds(16 * i, 16)
        for k in range(4):
            fm[:, 128 * k : 128 * k + 128] = ret[blocks, 16 * k : 16 * k + 16, :].reshape(256, 128)
        fo = ret[blocks, 64:72, :].astype(F32).reshape(128, 128).astype(BF16)
        values = []
        for (main, over), share in maps:
            lanes = slice(256 * i, 256 * i + 256)
            base = dot((main[:, lanes] == slot_main[:, lanes]).astype(BF16), fm[...])
            lanes = slice(128 * i, 128 * i + 128)
            hits = over[:, lanes] == slot_over[:, lanes]
            marks = [jnp.logical_and(hits, over_k[:, lanes] == k).astype(BF16) for k in range(4)]
            extra = [dot(mark, fo) for mark in marks]
            values.append((base, extra, share))
        return [
            sum(share * (base[:, 128 * k : 128 * k + 128] + extra[k]) for base, extra, share in values) for k in range(4)
        ]

    landed(s.at[pl.ds(0, 15)], b_r.at[0])
    for k, v in enumerate(pick_up(0)):
        acc[:, 128 * k : 128 * k + 128] = v
    landed(s.at[pl.ds(0, 16)], b_r.at[1])
    for k, v in enumerate(pick_up(1)):
        lanes = slice(128 * k, 128 * k + 128)
        out2[:, lanes] = (acc[:, lanes] + v).astype(BF16)

    left(s.at[pl.ds(0, NB - 1)], a_s)
    left(s.at[pl.ds(0, NB - NR * YN - 1)], a2_s)
    left(s.at[pl.ds(0, 30)], n_s)
    left(r.at[pl.ds(0, 2), pl.ds(0, 18)], g_s)
    left(s.at[pl.ds(0, (NR - 1) * YN)], y_s)
    left(s, v_s)
    left(r.at[pl.ds(0, 2)], d_s)
    left(s.at[pl.ds(0, NB - 1)], b_s)
    left(plx.at[pl.ds(0, 2)], p_s)
    left(plx.at[0], p2_s)
    left(wo.at[pl.ds(1, 3), piece], wo_s)
    left(wo.at[pl.ds(1, 3), pl.ds(0, 96)], wy_s)
    for copy in swaps + [shared, halo_copy]:
        copy.wait_send()


def local(
    first_input, first_gain, pool_inward, pool_mixing, pool_scale, pool_outward,
    second_input, second_gain, route_ids, route_logits, expert_gate, expert_up, expert_down,
):
    vmem = pl.BlockSpec(memory_space=pltpu.VMEM)
    far = pl.BlockSpec(memory_space=pl.ANY)
    dma = pltpu.SemaphoreType.DMA
    m = PAIR * 18
    return pl.pallas_call(
        kernel,
        name="mixer_experts",
        out_shape=(pltpu.VMEM((512, 512), BF16), pltpu.VMEM((256, 512), BF16)),
        in_specs=[far] * 13,
        out_specs=(vmem, vmem),
        scratch_shapes=[
            pltpu.VMEM((2, 256), jnp.int32),
            pltpu.VMEM((2048,), BF16),
            pltpu.VMEM((2048,), BF16),
            pltpu.VMEM((1, 256, 256), BF16),
            pltpu.VMEM((256,), BF16),
            pltpu.VMEM((2, 256), F32),
            pltpu.VMEM((512, 2048), BF16),
            pltpu.VMEM((2048, 256), BF16),
            pltpu.VMEM((256, 2048), BF16),
            pltpu.VMEM((2048, 512), BF16),
            pltpu.VMEM((2048, 512), BF16),
            pltpu.VMEM((1024, 2048), BF16),
            pltpu.VMEM((2048, 512), BF16),
            pltpu.VMEM((2048, 512), BF16),
            pltpu.VMEM((512, 2048), BF16),
            pltpu.VMEM((512, 256), BF16),
            pltpu.VMEM((528, 256), F32),
            pltpu.VMEM((16, 256), BF16),
            pltpu.VMEM((16, 256), BF16),
            pltpu.VMEM((4, 512, 256), BF16),
            pltpu.VMEM((4, 256, 512), BF16),
            pltpu.VMEM((4, 256, 512), BF16),
            pltpu.VMEM((NB, 72, 128), BF16),
            pltpu.VMEM((NB - NR * YN, 72, 128), BF16),
            pltpu.VMEM((NB - NR * YN, 72, 128), BF16),
            pltpu.VMEM((NB - NR * YN, 72, 128), BF16),
            pltpu.VMEM((4, NB, 72, 128), BF16),
            pltpu.VMEM((m, 2048), BF16),
            pltpu.VMEM((m, 1024), BF16),
            pltpu.VMEM((4, NB, 72, 128), BF16),
            pltpu.VMEM((2, NB, 72, 128), BF16),
            pltpu.VMEM((NB, 72, 128), BF16),
            pltpu.VMEM((NB, 72, 128), BF16),
            pltpu.VMEM((NB, 72, 128), BF16),
            pltpu.VMEM((256, 512), BF16),
            pltpu.VMEM((256, 512), F32),
            dma((13,)),
            dma((3,)), dma((3,)),
            dma, dma((6,)),
            dma, dma, dma((3,)),
            dma, dma((2 * NR,)),
            dma, dma,
            dma, dma((2, 4)),
            dma, dma((NG,)),
            dma, dma((2,)),
            dma, dma,
            dma, dma,
            dma, dma,
            dma, dma,
            dma, dma((2,)),
            dma, dma,
        ],
        compiler_params=pltpu.CompilerParams(
            collective_id=0, has_side_effects=True, vmem_limit_bytes=64000 * 1024
        ),
    )(
        first_input, first_gain, pool_inward, pool_mixing, pool_scale, pool_outward,
        second_input, second_gain, route_ids.T, route_logits.T, expert_gate, expert_up, expert_down,
    )


def solution(mesh):
    placed = (
        P("ep", None), P(), P(None, "tp"), P("tp", None, None), P("tp"), P("tp", None),
        P("ep", None), P(), P("ep", None), P("ep", None),
        P("ep", None, "tp"), P("ep", None, "tp"), P("ep", "tp", None),
    )
    return jax.shard_map(
        local, mesh=mesh, in_specs=placed, out_specs=(P("ep", "tp"), P("ep", "tp")), check_vma=False
    )
```

```python
import jax
import jax.numpy as jnp
from jax import lax
from jax.experimental import pallas as pl
from jax.experimental.pallas import tpu as pltpu
from jax.sharding import PartitionSpec as P

MESH = pl.DeviceIdType.MESH
F32, BF16 = jnp.float32, jnp.bfloat16
EPS = 1e-06
ZN, YN, XN = 8, 4, 4
NB = ZN * YN
NG = ZN
EP = NB * 2
PAIR = 2 * YN
ORDER = (3, 5, 4, 0, 2, 6, 1, 7)
NR = 3
SELF = 3 * YN


def dot(a, b):
    return jnp.dot(a, b, preferred_element_type=F32)


def dot_t(a, b):
    return lax.dot_general(a, b, (((0,), (0,)), ((), ())), preferred_element_type=F32)


def iota(shape, dim):
    return lax.broadcasted_iota(jnp.int32, shape, dim)


def group_dz(g):
    dz = jnp.full_like(g, ORDER[0])
    for i in range(1, NG):
        dz = jnp.where(g == i, ORDER[i], dz)
    return dz


def kernel(
    x1_h, g1_h, pin_h, pmix_h, psc_h, pout_h, x2_h, g2_h, ids_h, lg_h, wg_h, wu_h, wd_h,
    out1, out2,
    ids, g2, g1, pmix, psc, lg, x1, pin, x2, wg, wu, wd, wg2, wu2,
    n1, pl_in, ext, halo, tail, plx, wo, xq,
    s, s1, s2, s3, r, lhs, hid, tm, rr, rv, fin, ret, fm, acc,
    sem_in, ws_s, ws_r, a_s, a_r, a2_s, n_s, n_r, g_s, g_r, y_s, y_r, v_s, v_r, d_s, d_r,
    b_s, b_r, h_s, h_r, wo_s, wo_r, wy_s, wy_r, wp_s, wp_r, p_s, p_r, p2_s, p2_r,
):
    ep, t = lax.axis_index("ep"), lax.axis_index("tp")
    c = lax.rem(ep, 2)
    chip = ep // 2
    y, z = lax.rem(chip, YN), chip // YN

    def at(dz, dy, dc=0):
        z2, y2, c2 = (z + dz + ZN) & (ZN - 1), (y + dy + YN) & (YN - 1), (c + dc) & 1
        return ((z2 * YN + y2) * 2 + c2, t)

    def along(dx):
        return (ep, (t + dx) & (XN - 1))

    def quarter(dx):
        return (t + dx + XN) & (XN - 1)

    partner = at(0, 0, 1)
    following = (lax.rem(ep + 1, EP), t)
    previous = (lax.rem(ep + EP - 1, EP), t)

    def remote(src, dst, ss, rs, device):
        return pltpu.make_async_remote_copy(
            src_ref=src, dst_ref=dst, send_sem=ss, recv_sem=rs, device_id=device, device_id_type=MESH
        )

    def blocks_of(g, first=0, count=YN):
        return pl.ds(g * YN + first, count)

    loads = [
        pltpu.make_async_copy(a, b, sem_in.at[i])
        for i, (a, b) in enumerate(
            [(x2_h, x2), (x1_h, x1), (pin_h, pin), (wg_h.at[0], wg), (wu_h.at[0], wu), (wd_h.at[0], wd.at[pl.ds(0, 512)])]
        )
    ]
    small = [
        pltpu.make_async_copy(a, b, sem_in.at[7 + i])
        for i, (a, b) in enumerate([(ids_h, ids), (g2_h, g2), (g1_h, g1), (pmix_h, pmix), (psc_h, psc), (lg_h, lg)])
    ]
    for copy in small[:2] + loads[:1] + small[2:3] + loads[1:3] + small[3:]:
        copy.start()

    bar = pltpu.get_barrier_semaphore()

    for b in range(NB):
        if b != SELF:
            pl.semaphore_signal(bar, inc=1, device_id=at(ORDER[b // YN], b % YN), device_id_type=MESH)
    for dx in (1, 2, 3):
        pl.semaphore_signal(bar, inc=1, device_id=along(dx), device_id_type=MESH)
    pl.semaphore_signal(bar, inc=1, device_id=partner, device_id_type=MESH)
    pl.semaphore_signal(bar, inc=1, device_id=previous, device_id_type=MESH)

    small[0].wait()
    expert = iota((NB, 256), 0)
    one0 = (ids[0:1, :] == expert).astype(F32)
    one1 = (ids[1:2, :] == expert).astype(F32)
    earlier = (iota((256, 256), 0) < iota((256, 256), 1)).astype(BF16)
    place = dot((one0 + one1).astype(BF16), earlier) + 1.0

    def slot_maps(marks):
        held = (place * marks).astype(BF16)

        def spread(width, per):
            e, col = iota((NB, width), 0), iota((NB, width), 1) // per
            dz = group_dz(col // YN)
            hit = ((e // YN - z - dz + 2 * ZN) & (ZN - 1)) + ((lax.rem(e, YN) - y - lax.rem(col, YN) + 2 * YN) & (YN - 1))
            return dot_t(held, (hit == 0).astype(BF16))

        return spread(NB * 16, 16), spread(NB * 8, 8)

    slot_main = (lax.rem(iota((256, NB * 16), 1), 16) + 1).astype(F32)
    over_col = iota((256, NB * 8), 1)
    slot_over = (lax.rem(over_col // 4, 2) + 17).astype(F32)
    over_k = lax.rem(over_col, 4)

    small[1].wait()
    loads[0].wait()

    def norm2(i, carry):
        rows = pl.ds(pl.multiple_of(i * 64, 64), 64)
        v = x2[rows, :].astype(F32)
        inv = lax.rsqrt(jnp.mean(v * v, axis=-1, keepdims=True) + EPS)
        for dx in range(4):
            cols = pl.ds(pl.multiple_of(quarter(-dx) * 512, 512), 512)
            xq[dx, rows, :] = (x2[rows, cols].astype(F32) * inv * g2[cols].astype(F32)).astype(BF16)
        return carry

    lax.fori_loop(0, 4, norm2, 0)
    in_main, in_over = slot_maps(one0 + one1)
    pick_main = (in_main == slot_main).astype(BF16)
    picks_over = [jnp.logical_and(in_over == slot_over, over_k == k).astype(BF16) for k in range(4)]

    def fill(buf, dx, skip):
        xv = xq[dx]
        count = NB - skip
        rows_main = dot_t(pick_main[:, skip * 16 :], xv)
        rows_over = jnp.zeros((count * 8, 128), F32)
        for k in range(4):
            lanes = slice(128 * k, 128 * k + 128)
            buf[:, 16 * k : 16 * k + 16, :] = rows_main[:, lanes].reshape(count, 16, 128).astype(BF16)
            rows_over = rows_over + dot_t(picks_over[k][:, skip * 8 :], xv[:, lanes])
        buf[:, 64:72, :] = rows_over.reshape(count, 8, 128).astype(BF16)
        r[dx, SELF] = buf[SELF - skip]

    fill(s, 0, 0)

    small[2].wait()
    loads[1].wait()
    loads[2].wait()

    def normed1(rows):
        v = x1[rows, :].astype(F32)
        inv = lax.rsqrt(jnp.mean(v * v, axis=-1, keepdims=True) + EPS)
        return (v * inv * g1[...].astype(F32)).astype(BF16)

    tail[...] = dot(normed1(pl.ds(496, 16)), pin[...]).astype(BF16)
    halo_copy = remote(tail, halo, h_s, h_r, following)

    pl.semaphore_wait(bar, NB - 1 + 3 + 2)

    halo_copy.start()

    def toward(b):
        return at(group_dz(b // YN), lax.rem(b, YN))

    def send_blocks(buf, dx, skip, g, ss, arrival):
        def body(dy, carry):
            b = g * YN + dy
            remote(buf.at[b - skip], r.at[dx, b], ss, arrival, at(ORDER[g], dy)).start()
            return carry

        lax.fori_loop(1 if ORDER[g] == 0 else 0, YN, body, 0)

    half_rows = pl.ds(pl.multiple_of(c * 128, 128), 128)
    piece = pl.ds(pl.multiple_of(c * 128 + y * 32, 32), 32)
    outward = []
    for dx in (1, 2, 3):
        cols = pl.ds(pl.multiple_of(quarter(dx) * 512, 512), 512)
        outward.append(remote(pout_h.at[piece, cols], wo.at[dx, piece], wo_s, wo_r, along(dx)))
    for copy in outward:
        copy.start()
    along_y = [
        remote(wo.at[pl.ds(1, 3), piece], wo.at[pl.ds(1, 3), piece], wy_s, wy_r, at(0, dy)) for dy in (1, 2, 3)
    ]
    shared = remote(wo.at[pl.ds(1, 3), half_rows], wo.at[pl.ds(1, 3), half_rows], wp_s, wp_r, partner)
    for g in range(NR):
        send_blocks(s, 0, 0, g, a_s, a_r.at[g])
    send_blocks(s, 0, 0, NR, a_s, n_r.at[0])

    swaps = [
        remote(a, b, ws_s.at[i], ws_r.at[i], partner)
        for i, (a, b) in enumerate([(wg_h.at[0], wg2), (wu_h.at[0], wu2), (wd_h.at[0], wd.at[pl.ds(512, 512)])])
    ]
    for copy in swaps + loads[3:]:
        copy.start()

    own_out = pltpu.make_async_copy(
        pout_h.at[:, pl.ds(pl.multiple_of(t * 512, 512), 512)], wo.at[0], sem_in.at[6]
    )
    own_out.start()

    def landed(ref, sem):
        remote(ref, ref, a_s, sem, partner).wait_recv()

    def left(ref, sem):
        remote(ref, ref, sem, a_r.at[0], partner).wait_send()

    def gather(g, dx):
        rows = blocks_of(g)
        arrival = g_r.at[2 * g + dx // 2 if g < NR - 1 else g // 4 + 2 * NR - 2]
        return remote(r.at[0, rows], r.at[dx, rows], g_s, arrival, along(dx))

    def relay(g, dx):
        rows = blocks_of(g, dx - 1, 2)
        return remote(r.at[dx, rows], r.at[2, rows], y_s, y_r, along(dx))

    def arrived(g):
        landed(s.at[pl.ds(0, YN)], a_r.at[g])

    def pass_on(g):
        arrived(g)
        for dx in ((1, 3), (1, 3), (1, 3, 2), (), (3,), (1,))[g]:
            gather(g, dx).start()

    def relay_on(g):
        for dx in (1, 3):
            gather(g, dx).wait_recv()
            relay(g, dx).start()

    def norm1(i, carry):
        rows = pl.ds(pl.multiple_of(i * 64, 64), 64)
        n1[rows, :] = normed1(rows)
        return carry

    lax.fori_loop(0, 8, norm1, 0)
    def inward(i, carry):
        rows = pl.ds(pl.multiple_of(i * 256, 256), 256)
        pl_in[rows, :] = dot(n1[rows, :], pin[...]).astype(BF16)
        return carry

    lax.fori_loop(0, 2, inward, 0)

    for copy in small[3:]:
        copy.wait()
    halo_copy.wait_recv()
    ext[0:16, :] = jnp.where(ep == 0, 0.0, halo[...].astype(F32))
    ext[16:528, :] = pl_in[...].astype(F32)
    window = jnp.left_shift(jnp.int32(2), t)
    reach = ext[...]
    total = jnp.zeros((528, 256), F32)
    for i in range(4):
        reach = reach + pltpu.roll(reach, 1 << i, 0)
        total = jnp.where(t == i, reach, total)
    count = jnp.minimum(ep * 512 + iota((512, 1), 0) + 1, window).astype(F32)
    mixed = (total[16:528, :] / count - ext[16:528, :]).astype(BF16)
    plx[0] = (dot(mixed, pmix[0]) * psc[...].astype(F32)).astype(BF16)
    def pooled(dx):
        return remote(plx.at[0], plx.at[dx], p_s, p_r.at[dx // 2], along(dx))

    def pooled_on(dx):
        rows = pl.ds(128 * (dx - 1), 256)
        return remote(plx.at[dx, rows], plx.at[2, rows], p2_s, p2_r, along(dx))

    for dx in (1, 3):
        pooled(dx).start()

    for dx in (1, 2, 3):
        fill((s1, s2, s3)[dx - 1], dx, NR * YN)
    for g in (3, 4, 5, 6, 7):
        whole = ORDER[g] in (0, 1, 7)
        for buf, dx, ss in ((s, 0, a_s), (s2, 2, a2_s), (s1, 1, n_s), (s3, 3, n_s)):
            if dx == 0 and g > NR:
                send_blocks(s, 0, 0, g, a_s, n_r.at[2] if whole else a_r.at[g])
            elif dx == 2 or (dx and whole) or (g, dx) in ((4, 1), (5, 3)):
                send_blocks(buf, dx, NR * YN, g, ss, n_r.at[0 if g == NR else 2 if whole else 1])
    pass_on(0)
    pass_on(1)
    relay_on(0)
    relay_on(1)
    pass_on(2)
    pass_on(4)
    pass_on(5)
    landed(wo.at[pl.ds(1, 3), piece], wo_r)
    for copy in along_y:
        copy.start()

    def expand(k):
        m, n = iota((PAIR * 2, PAIR * 8), 0), iota((PAIR * 2, PAIR * 8), 1)
        return (n == (m // 2) * 8 + lax.rem(m, 2) * 4 + k).astype(BF16)

    def rows_in(i):
        blocks = pl.ds(i * PAIR, PAIR)
        for dx in range(4):
            q = quarter(-dx)
            over = r[dx, blocks, 64:72, :].astype(F32).reshape(PAIR * 8, 128).astype(BF16)
            for k in range(4):
                cols = pl.ds(pl.multiple_of(q * 512 + 128 * k, 128), 128)
                lhs[0 : PAIR * 16, cols] = r[dx, blocks, 16 * k : 16 * k + 16, :].reshape(PAIR * 16, 128)
                lhs[PAIR * 16 : PAIR * 18, cols] = dot(expand(k), over).astype(BF16)

    def units(n, carry):
        cols = pl.ds(n * 256, 256) if isinstance(n, int) else pl.ds(pl.multiple_of(n * 256, 256), 256)
        for j, (a, b) in enumerate([(wg, wu), (wg2, wu2)]):
            gate, up = dot(lhs[...], a[:, cols]), dot(lhs[...], b[:, cols])
            hid[:, pl.ds(512 * j + n * 256, 256) if isinstance(n, int) else pl.ds(pl.multiple_of(512 * j + n * 256, 256), 256)] = (gate / (1.0 + jnp.exp(-gate)) * up).astype(BF16)
        return carry

    def down(i, dx):
        blocks = pl.ds(i * PAIR, PAIR)
        cols = pl.ds(pl.multiple_of(quarter(dx) * 512, 512), 512)
        term = dot(hid[...], wd[:, cols])
        n, m = iota((PAIR * 8, PAIR * 2), 0), iota((PAIR * 8, PAIR * 2), 1)
        spread = dot((n // 4 == m).astype(BF16), term[PAIR * 16 :].astype(BF16))
        lane_group = lax.rem(iota((PAIR * 8, 128), 0), 4)
        over = spread[:, 0:128]
        for k in range(4):
            part = term[0 : PAIR * 16, 128 * k : 128 * k + 128]
            tm[dx, blocks, 16 * k : 16 * k + 16, :] = part.reshape(PAIR, 16, 128).astype(BF16)
            if k:
                over = jnp.where(lane_group == k, spread[:, 128 * k : 128 * k + 128], over)
        tm[dx, blocks, 64:72, :] = over.reshape(PAIR, 8, 128).astype(BF16)

    def by_way(j, dx):
        rows = blocks_of(2 * j + dx // 2)
        return remote(tm.at[2, rows], rv.at[rows], v_s, v_r.at[dx // 2, j], along(dx))

    def direct(j, dx):
        g = 2 * j + 1 - dx // 2
        rows = blocks_of(g)
        return remote(tm.at[dx, rows], rr.at[dx // 2, rows], d_s, d_r.at[g], along(dx))

    def joined(j, dx):
        g = 2 * j + dx // 2
        rows = blocks_of(g)
        return remote(tm.at[dx, rows], rr.at[dx // 2, rows], d_s, d_r.at[g], along(dx))

    def each(first, last, action):
        def body(g, carry):
            action(g)
            return carry

        lax.fori_loop(first, last, body, 0)

    def start_by_way(j):
        for dx in (1, 3):
            by_way(j, dx).start()

    def join(j):
        for dx in (1, 3):
            by_way(j, dx).wait_recv()
            rows = blocks_of(2 * j + dx // 2)
            tm[dx, rows] = (tm[dx, rows].astype(F32) + rv[rows].astype(F32)).astype(BF16)
            joined(j, dx).start()

    def back(b):
        return remote(fin.at[b], ret.at[b], b_s, b_r.at[b // (4 * YN)], at(ZN - group_dz(b // YN), YN - lax.rem(b, YN)))

    def summed(g):
        rows = blocks_of(g)
        landed(s.at[pl.ds(0, 2 * YN)], d_r.at[g])
        v = tm[0, rows].astype(F32) + rr[0, rows].astype(F32) + rr[1, rows].astype(F32)
        fin[rows] = v.astype(BF16)

    def give_back(g):
        summed(g)
        for dy in range(YN):
            back(g * YN + dy).start()

    def up_part(j):
        with jax.named_scope(f"rows{j}"):
            rows_in(j)
        with jax.named_scope(f"units{j}"):
            lax.fori_loop(0, 2, units, 0)

    def down_part(j):
        with jax.named_scope(f"down{j}"):
            down(j, 2)
            start_by_way(j)
            for dx in (1, 3, 0):
                down(j, dx)
            for dx in (1, 3):
                direct(j, dx).start()

    landed(s.at[pl.ds(0, PAIR)], y_r)
    for copy in loads[3:]:
        copy.wait()
    for copy in swaps:
        copy.wait_recv()
    up_part(0)
    down_part(0)
    landed(s.at[pl.ds(0, NR * YN)], g_r.at[2 * NR - 2])
    landed(s.at[pl.ds(0, NR * YN)], n_r.at[0])
    up_part(1)
    down_part(1)
    join(0)
    landed(s.at[pl.ds(0, PAIR)], g_r.at[2 * NR - 1])
    landed(s.at[pl.ds(0, 4 * YN)], n_r.at[1])
    up_part(2)
    down_part(2)
    join(1)
    landed(wo.at[pl.ds(1, 3), pl.ds(0, 96)], wy_r)
    shared.start()
    landed(s, n_r.at[2])
    up_part(3)
    each(0, 2, give_back)
    down_part(3)
    join(2)
    give_back(2)
    summed(NR)
    ret[SELF] = fin[SELF]
    for dy in range(1, YN):
        back(SELF + dy).start()
    join(3)
    for dx in (1, 3):
        pooled(dx).wait_recv()
        pooled_on(dx).start()
    each(4, NG, give_back)

    row0 = iota((8, 256), 0) == 0
    gap = lg[1:2, :] - lg[0:1, :]
    shares = jnp.where(row0, 1.0 / (1.0 + jnp.exp(gap)), 1.0 / (1.0 + jnp.exp(-gap))).T
    maps = [(slot_maps(one0), shares[:, 0:1]), (slot_maps(one1), shares[:, 1:2])]
    own_out.wait()
    shared.wait_recv()
    landed(plx.at[0], p2_r)
    for n in range(2):
        rows = slice(256 * n, 256 * n + 256)
        mixed_out = dot(plx[0, rows, :], wo[0])
        for dx in (1, 2, 3):
            mixed_out = mixed_out + dot(plx[dx, rows, :], wo[dx])
        out1[rows, :] = mixed_out.astype(BF16)

    def pick_up(i):
        blocks = pl.ds(16 * i, 16)
        for k in range(4):
            fm[:, 128 * k : 128 * k + 128] = ret[blocks, 16 * k : 16 * k + 16, :].reshape(256, 128)
        fo = ret[blocks, 64:72, :].astype(F32).reshape(128, 128).astype(BF16)
        values = []
        for (main, over), share in maps:
            lanes = slice(256 * i, 256 * i + 256)
            base = dot((main[:, lanes] == slot_main[:, lanes]).astype(BF16), fm[...])
            lanes = slice(128 * i, 128 * i + 128)
            hits = over[:, lanes] == slot_over[:, lanes]
            marks = [jnp.logical_and(hits, over_k[:, lanes] == k).astype(BF16) for k in range(4)]
            extra = [dot(mark, fo) for mark in marks]
            values.append((base, extra, share))
        return [
            sum(share * (base[:, 128 * k : 128 * k + 128] + extra[k]) for base, extra, share in values) for k in range(4)
        ]

    landed(s.at[pl.ds(0, 15)], b_r.at[0])
    for k, v in enumerate(pick_up(0)):
        acc[:, 128 * k : 128 * k + 128] = v
    landed(s.at[pl.ds(0, 16)], b_r.at[1])
    for k, v in enumerate(pick_up(1)):
        lanes = slice(128 * k, 128 * k + 128)
        out2[:, lanes] = (acc[:, lanes] + v).astype(BF16)

    left(s.at[pl.ds(0, NB - 1)], a_s)
    left(s.at[pl.ds(0, NB - NR * YN - 1)], a2_s)
    left(s.at[pl.ds(0, 30)], n_s)
    left(r.at[pl.ds(0, 2), pl.ds(0, 18)], g_s)
    left(s.at[pl.ds(0, (NR - 1) * YN)], y_s)
    left(s, v_s)
    left(r.at[pl.ds(0, 2)], d_s)
    left(s.at[pl.ds(0, NB - 1)], b_s)
    left(plx.at[pl.ds(0, 2)], p_s)
    left(plx.at[0], p2_s)
    left(wo.at[pl.ds(1, 3), piece], wo_s)
    left(wo.at[pl.ds(1, 3), pl.ds(0, 96)], wy_s)
    for copy in swaps + [shared, halo_copy]:
        copy.wait_send()


def local(
    first_input, first_gain, pool_inward, pool_mixing, pool_scale, pool_outward,
    second_input, second_gain, route_ids, route_logits, expert_gate, expert_up, expert_down,
):
    vmem = pl.BlockSpec(memory_space=pltpu.VMEM)
    far = pl.BlockSpec(memory_space=pl.ANY)
    dma = pltpu.SemaphoreType.DMA
    m = PAIR * 18
    return pl.pallas_call(
        kernel,
        name="mixer_experts",
        out_shape=(pltpu.VMEM((512, 512), BF16), pltpu.VMEM((256, 512), BF16)),
        in_specs=[far] * 13,
        out_specs=(vmem, vmem),
        scratch_shapes=[
            pltpu.VMEM((2, 256), jnp.int32),
            pltpu.VMEM((2048,), BF16),
            pltpu.VMEM((2048,), BF16),
            pltpu.VMEM((1, 256, 256), BF16),
            pltpu.VMEM((256,), BF16),
            pltpu.VMEM((2, 256), F32),
            pltpu.VMEM((512, 2048), BF16),
            pltpu.VMEM((2048, 256), BF16),
            pltpu.VMEM((256, 2048), BF16),
            pltpu.VMEM((2048, 512), BF16),
            pltpu.VMEM((2048, 512), BF16),
            pltpu.VMEM((1024, 2048), BF16),
            pltpu.VMEM((2048, 512), BF16),
            pltpu.VMEM((2048, 512), BF16),
            pltpu.VMEM((512, 2048), BF16),
            pltpu.VMEM((512, 256), BF16),
            pltpu.VMEM((528, 256), F32),
            pltpu.VMEM((16, 256), BF16),
            pltpu.VMEM((16, 256), BF16),
            pltpu.VMEM((4, 512, 256), BF16),
            pltpu.VMEM((4, 256, 512), BF16),
            pltpu.VMEM((4, 256, 512), BF16),
            pltpu.VMEM((NB, 72, 128), BF16),
            pltpu.VMEM((NB - NR * YN, 72, 128), BF16),
            pltpu.VMEM((NB - NR * YN, 72, 128), BF16),
            pltpu.VMEM((NB - NR * YN, 72, 128), BF16),
            pltpu.VMEM((4, NB, 72, 128), BF16),
            pltpu.VMEM((m, 2048), BF16),
            pltpu.VMEM((m, 1024), BF16),
            pltpu.VMEM((4, NB, 72, 128), BF16),
            pltpu.VMEM((2, NB, 72, 128), BF16),
            pltpu.VMEM((NB, 72, 128), BF16),
            pltpu.VMEM((NB, 72, 128), BF16),
            pltpu.VMEM((NB, 72, 128), BF16),
            pltpu.VMEM((256, 512), BF16),
            pltpu.VMEM((256, 512), F32),
            dma((13,)),
            dma((3,)), dma((3,)),
            dma, dma((6,)),
            dma, dma, dma((3,)),
            dma, dma((2 * NR,)),
            dma, dma,
            dma, dma((2, 4)),
            dma, dma((NG,)),
            dma, dma((2,)),
            dma, dma,
            dma, dma,
            dma, dma,
            dma, dma,
            dma, dma((2,)),
            dma, dma,
        ],
        compiler_params=pltpu.CompilerParams(
            collective_id=0, has_side_effects=True, vmem_limit_bytes=64000 * 1024
        ),
    )(
        first_input, first_gain, pool_inward, pool_mixing, pool_scale, pool_outward,
        second_input, second_gain, route_ids.T, route_logits.T, expert_gate, expert_up, expert_down,
    )


def solution(mesh):
    placed = (
        P("ep", None), P(), P(None, "tp"), P("tp", None, None), P("tp"), P("tp", None),
        P("ep", None), P(), P("ep", None), P("ep", None),
        P("ep", None, "tp"), P("ep", None, "tp"), P("ep", "tp", None),
    )
    return jax.shard_map(
        local, mesh=mesh, in_specs=placed, out_specs=(P("ep", "tp"), P("ep", "tp")), check_vma=False
    )
```
